32 devices in a mesh: grp: 2 (over y), sp: 4 (over z), tp: 4 (over x, core).
Axes of the slice: x: 2, y: 2, z: 4, core: 2. Of those that a mesh axis runs over, the one named last changes fastest.
Arguments:
- latent: bfloat16 [3072, 4096], P(('grp', 'sp')), parts along dimension 0, may hold values from -6 to 6
- context: bfloat16 [512, 4096], P(('grp', 'sp')), parts along dimension 0, may hold values from -6 to 6
- cond_latent: bfloat16 [8192], P('grp'), parts along dimension 0, may hold values from -6 to 6
- cond_context: bfloat16 [4096], replicated, may hold values from -6 to 6
- w_shift: bfloat16 [4096, 4096], P('sp', 'tp'), may hold values from -0.09375 to 0.09375
- w_scale: bfloat16 [4096, 4096], P('sp', 'tp'), may hold values from -0.09375 to 0.09375
- w_gate: bfloat16 [4096, 4096], P('sp', 'tp'), may hold values from -0.1875 to 0.1875
- norm_gain: float32 [4096], replicated, may hold values from 0.1 to 1.9
- w_query: bfloat16 [4096, 2048], P(None, 'tp'), may hold values from -0.09375 to 0.09375
- w_key: bfloat16 [4096, 1024], P(None, 'tp'), may hold values from -0.09375 to 0.09375
- w_value: bfloat16 [4096, 1024], P(None, 'tp'), may hold values from -0.09375 to 0.09375
- q_gain: float32 [128], replicated, may hold values from 1 to 6.5, as said below
- k_gain: float32 [128], replicated, may hold values from 1 to 6.5, as said below
- w_out: bfloat16 [2048, 4096], P('tp'), may hold values from -0.5 to 0.5
Outputs:
- mixed: bfloat16 [3072, 4096], P(('grp', 'sp', 'tp')), parts along dimension 0
The draws below stay inside these ranges and needn't reach their ends.
There are 2 independent parts, one for each index of `grp`. The reference program is written for one: setup_inputs(seed, part) draws one part's arguments, and reference() takes and returns one part's arrays. A program takes and returns all parts, laid end to end along the dimension named above; an argument that names none is the same for every part. Nothing has to cross between parts.
Inputs may be any that keep to these rules, and one draw needn't show every extreme that they name: `q_gain`: positive gains. `k_gain`: positive gains.
All inputs are finite; a program needn't handle non-finite values.
Results may differ from the reference program's by a relative error of at most 0.015.
The reference program's roundings to bfloat16 on the way (of `cond_act`, `normed`, `ctx_normed`, `queries`, `weights` and `attended`) count: a program that leaves them out, or rounds other values in their place, can miss the bound.
Values may be sent and summed in bfloat16 or wider, within the bound.
A program may use at most 128 MiB of HBM per device.

```python
import math
import jax
import jax.numpy as jnp
from jax import lax

D = 4096
HEADS = 16
KV_HEADS = 8
HEAD = 128
GRID_W = 64
TOK_DEV = 384
CTX = 256
TOKENS = 1536
N_TP = 4


def gain_draw(key):
    return jnp.exp(jax.random.uniform(key, (HEAD,), jnp.float32, 0.0, math.log(2.5)))


def draw_q_gain(key, part):
    return gain_draw(jax.random.fold_in(key, 11))


def draw_k_gain(key, part):
    return gain_draw(jax.random.fold_in(key, 23))


def level_of(own_key, shape, cuts, least, high):
    def one(position, shards_of):
        steps = jax.random.uniform(jax.random.fold_in(jax.random.fold_in(own_key, 6), position), (shards_of,), jnp.float32, least / len(cuts), high / len(cuts))
        return jnp.repeat(jnp.exp(steps), shape[position] // shards_of).reshape((-1,) + (1,) * (len(shape) - position - 1))

    factor_of = one(*cuts[0])
    for cut in cuts[1:]:
        factor_of = factor_of * one(*cut)
    return factor_of


def noise(rng, shape, deviation, bound, cuts=(), kind=jnp.bfloat16):
    level = level_of(rng, shape, cuts, -0.22, 0.18) if cuts else 1.0
    drawn = jax.random.normal(rng, shape, jnp.float32) * deviation * level
    return jnp.minimum(jnp.maximum(drawn, -bound), bound).astype(kind)


def setup_inputs(seed: int = 0, part: int = 0) -> dict:
    seeds = jax.random.split(jax.random.key(seed), 15)
    part_keys = jax.random.split(jax.random.fold_in(seeds[14], part), 15)
    latent = noise(part_keys[0], (TOKENS, D), 1.0, 6.0, ((0, 4),))
    context = noise(part_keys[1], (CTX, D), 1.0, 6.0, ((0, 4),))
    cond_latent = noise(part_keys[2], (D,), 1.0, 6.0)
    cond_context = noise(seeds[3], (D,), 1.0, 6.0)
    w_shift = noise(seeds[4], (D, D), D ** -0.5, 0.09375, ((0, 4), (1, 4)))
    w_scale = noise(seeds[5], (D, D), D ** -0.5, 0.09375, ((0, 4), (1, 4)))
    w_gate = noise(seeds[6], (D, D), (D // 4) ** -0.5, 0.1875, ((0, 4), (1, 4)))
    norm_gain = jnp.clip(1.0 + 0.18 * jax.random.normal(seeds[7], (D,), jnp.float32), 0.1, 1.9)
    w_query = noise(seeds[8], (D, HEADS * HEAD), D ** -0.5, 0.09375, ((1, 4),))
    w_key = noise(seeds[9], (D, KV_HEADS * HEAD), D ** -0.5, 0.09375, ((1, 4),))
    w_value = noise(seeds[10], (D, KV_HEADS * HEAD), D ** -0.5, 0.09375, ((1, 4),))
    q_gain = draw_q_gain(jax.random.fold_in(seeds[14], 71), part)
    k_gain = draw_k_gain(jax.random.fold_in(seeds[14], 71), part)
    w_out = noise(seeds[13], (HEADS * HEAD, D), HEAD ** -0.5, 0.5, ((0, 4),))
    return dict(latent=latent, context=context, cond_latent=cond_latent, cond_context=cond_context, w_shift=w_shift, w_scale=w_scale, w_gate=w_gate, norm_gain=norm_gain, w_query=w_query, w_key=w_key, w_value=w_value, q_gain=q_gain, k_gain=k_gain, w_out=w_out)


epsilon = 1e-06
context_lift = 1.5
rope_theta = 10000.0

def rms_rows(values, gain):
    values = values.astype(jnp.float32)
    return values * lax.rsqrt(lax.optimization_barrier(jnp.mean(values * values, axis=-1, keepdims=True)) + epsilon) * gain

def rotate(values, positions):
    count, heads_here = (values.shape[0], values.shape[1])
    grid_row = (positions // GRID_W).astype(jnp.float32)
    grid_col = (positions % GRID_W).astype(jnp.float32)
    freqs = HEAD // 4
    inverse = rope_theta ** (-jnp.arange(freqs, dtype=jnp.float32) / freqs)
    angles = jnp.stack([grid_row, grid_col], axis=-1)[:, :, None] * inverse
    cosine = jnp.cos(angles)[:, None]
    sine = jnp.sin(angles)[:, None]
    split = values.reshape(count, heads_here, 2, 2, freqs)
    first_half = split[..., 0, :]
    second_half = split[..., 1, :]
    turned = jnp.stack([first_half * cosine - second_half * sine, first_half * sine + second_half * cosine], axis=-2)
    return turned.reshape(count, heads_here, HEAD)

def reference(latent, context, cond_latent, cond_context, w_shift, w_scale, w_gate, norm_gain, w_query, w_key, w_value, q_gain, k_gain, w_out):
    cond_act = jax.nn.silu(jnp.stack([cond_latent, cond_context]).astype(jnp.float32)).astype(jnp.bfloat16)
    shift = jnp.dot(cond_act, w_shift, preferred_element_type=jnp.float32)
    scale = jnp.dot(cond_act, w_scale, preferred_element_type=jnp.float32)
    gate = jnp.dot(cond_act, w_gate, preferred_element_type=jnp.float32)
    normed = (rms_rows(latent, norm_gain) * (1.0 + scale[0]) + shift[0]).astype(jnp.bfloat16)
    ctx_normed = (rms_rows(context, norm_gain) * (1.0 + scale[1]) + shift[1]).astype(jnp.bfloat16)
    positions = jnp.arange(TOKENS, dtype=jnp.int32)
    group = HEADS // KV_HEADS
    queries = jnp.dot(normed, w_query, preferred_element_type=jnp.float32).reshape(TOKENS, HEADS, HEAD)
    queries = rotate(rms_rows(queries, q_gain), positions).astype(jnp.bfloat16)
    keys = jnp.dot(normed, w_key, preferred_element_type=jnp.float32).reshape(TOKENS, KV_HEADS, HEAD)
    keys = rotate(rms_rows(keys, k_gain), positions).astype(jnp.bfloat16)
    values = jnp.dot(normed, w_value, preferred_element_type=jnp.float32).astype(jnp.bfloat16).reshape(TOKENS, KV_HEADS, HEAD)
    ctx_keys = jnp.dot(ctx_normed, w_key, preferred_element_type=jnp.float32).reshape(CTX, KV_HEADS, HEAD)
    ctx_keys = rms_rows(ctx_keys, k_gain).astype(jnp.bfloat16)
    ctx_values = jnp.dot(ctx_normed, w_value, preferred_element_type=jnp.float32).astype(jnp.bfloat16).reshape(CTX, KV_HEADS, HEAD)
    keys_f = keys.astype(jnp.float32)
    values_f = values.astype(jnp.float32)
    ctx_keys_f = ctx_keys.astype(jnp.float32)
    ctx_values_f = ctx_values.astype(jnp.float32)
    scaling = HEAD ** (-0.5)
    blocks = queries.reshape(TOKENS // TOK_DEV, TOK_DEV, KV_HEADS, group, HEAD)

    def attend(block):
        block_f = block.astype(jnp.float32)
        scores = jnp.einsum('qkgd,skd->kgqs', block_f, keys_f) * scaling
        ctx_scores = jnp.einsum('qkgd,ckd->kgqc', block_f, ctx_keys_f) * scaling + context_lift
        top = jnp.maximum(lax.optimization_barrier(jnp.max(scores, axis=-1)), lax.optimization_barrier(jnp.max(ctx_scores, axis=-1)))
        weights = jnp.exp(scores - top[..., None])
        ctx_weights = jnp.exp(ctx_scores - top[..., None])
        total = lax.optimization_barrier(jnp.sum(weights, axis=-1)) + lax.optimization_barrier(jnp.sum(ctx_weights, axis=-1))
        numerator = jnp.einsum('kgqs,skd->qkgd', weights.astype(jnp.bfloat16).astype(jnp.float32), values_f)
        numerator = numerator + jnp.einsum('kgqc,ckd->qkgd', ctx_weights.astype(jnp.bfloat16).astype(jnp.float32), ctx_values_f)
        return (numerator / jnp.transpose(total, (2, 0, 1))[..., None]).astype(jnp.bfloat16)
    attended = lax.map(attend, blocks).reshape(TOKENS, HEADS * HEAD)
    columns = HEADS * HEAD // N_TP
    heads_out = jnp.zeros((TOKENS, D), jnp.float32)
    for member in range(N_TP):
        partial_out = jnp.dot(attended[:, member * columns:(member + 1) * columns], w_out[member * columns:(member + 1) * columns], preferred_element_type=jnp.float32)
        rounded = lax.optimization_barrier(partial_out.astype(jnp.bfloat16))
        heads_out = heads_out + rounded.astype(jnp.float32)
    return (gate[0] * heads_out).astype(jnp.bfloat16)
```

```python
import functools
import math

import jax
import jax.numpy as jnp
from jax import lax
from jax.experimental import pallas as pl
from jax.experimental.pallas import tpu as pltpu
from jax.sharding import PartitionSpec as P

HEADS = 16
KV_HEADS = 8
HEAD = 128
GRID_W = 64
GROUP = HEADS // KV_HEADS

epsilon = 1e-06
context_lift = 1.5
rope_theta = 10000.0

MESH = pl.DeviceIdType.MESH
f32 = jnp.float32
bf16 = jnp.bfloat16


def tile_of(rows, most):
    best = 16
    for size in range(16, most + 1, 16):
        if rows % size == 0:
            best = size
    return best


def kernel(
    n_grp,
    n_sp,
    n_tp,
    tok,
    ctx,
    share,
    cond_latent_ref,
    cond_context_ref,
    gain_ref,
    q_gain_ref,
    k_gain_ref,
    latent_hbm,
    context_hbm,
    w_shift_hbm,
    w_scale_hbm,
    w_gate_hbm,
    w_query_hbm,
    w_key_hbm,
    w_value_hbm,
    w_out_hbm,
    out_ref,
    act_ref,
    x,
    w_mod,
    w_query,
    w_key,
    w_value,
    w_all,
    w_rest,
    inv,
    cos_ref,
    sin_a_ref,
    sin_b_ref,
    part,
    part_in,
    summed,
    mod,
    gate_part,
    gate_in,
    gate_sum,
    gate_mod,
    queries,
    kv,
    top,
    total,
    acc,
    attended,
    att_all,
    acc_out,
    pair_out,
    pair_in,
    mine,
    far_out,
    far_in,
    load_sem,
    mod_send,
    mod_recv,
    mod2_send,
    mod2_recv,
    gate_send,
    gate_recv,
    gate2_send,
    gate2_recv,
    right_send,
    right_recv,
    left_send,
    left_recv,
    pair_send,
    pair_recv,
    far_send,
    far_recv,
    own_send,
    own_recv,
    across_send,
    across_recv,
    beside_send,
    beside_recv,
    over_send,
    over_recv,
    last_send,
    last_recv,
    att_send,
    att_recv,
):
    grp = lax.axis_index("grp")
    sp = lax.axis_index("sp")
    tp = lax.axis_index("tp")
    chips = n_tp // 2
    chip = tp // 2
    core = lax.rem(tp, 2)
    partner = chip * 2 + 1 - core
    piece = tok // n_tp
    turns = w_all.shape[2] // (n_grp * share)
    shared = w_all.shape[2]
    rows = tok + ctx
    depth = x.shape[1]
    mod_cols = mod.shape[2]
    heads = queries.shape[1] // HEAD
    kv_cols = kv.shape[2] // 2
    kv_heads = kv_cols // HEAD
    kv_tile = tile_of(rows, 128)
    kv_chunks = rows // kv_tile
    per_unit = 2 if kv_chunks % 2 == 0 else 1
    units = kv_chunks // per_unit
    unit_rows = kv_tile * per_unit

    loads = {}

    def load(name, index, source, target):
        loads[name] = pltpu.make_async_copy(source, target, load_sem.at[index])
        loads[name].start()

    load("shift", 0, w_shift_hbm, w_mod.at[0])
    load("scale", 1, w_scale_hbm, w_mod.at[1])
    load("latent", 3, latent_hbm, x.at[pl.ds(0, tok)])
    load("context", 4, context_hbm, x.at[pl.ds(tok, ctx)])

    barrier = pltpu.get_barrier_semaphore()
    for k in range(1, n_sp):
        pl.semaphore_signal(
            barrier, inc=1, device_id={"sp": lax.rem(sp + k, n_sp)}, device_id_type=MESH
        )
    for k in range(1, n_tp):
        pl.semaphore_signal(
            barrier, inc=1, device_id={"tp": lax.rem(tp + k, n_tp)}, device_id_type=MESH
        )

    for k in range(1, n_grp):
        pl.semaphore_signal(
            barrier, inc=1, device_id={"grp": lax.rem(grp + k, n_grp)}, device_id_type=MESH
        )

    def tables(i, carry):
        at = pl.ds(pl.multiple_of(i * 16, 16), 16)
        index = i * 16 + lax.broadcasted_iota(jnp.int32, (16, HEAD), 0)
        lane = lax.broadcasted_iota(jnp.int32, (16, HEAD), 1)
        freqs = HEAD // 4
        position = sp * tok + index
        inverse = jnp.exp(lax.rem(lane, freqs).astype(f32) * (-math.log(rope_theta) / freqs))
        place = jnp.where(lane < 2 * freqs, lax.div(position, GRID_W), lax.rem(position, GRID_W))
        angle = jnp.where(index < tok, place.astype(f32) * inverse, 0.0)
        sine = jnp.sin(angle)
        first_half = lax.rem(lax.div(lane, freqs), 2) == 0
        cos_ref[at, :] = jnp.cos(angle)
        sin_a_ref[at, :] = jnp.where(first_half, -sine, 0.0)
        sin_b_ref[at, :] = jnp.where(first_half, 0.0, sine)
        return carry

    lax.fori_loop(0, rows // 16, tables, 0)
    mod_rows = w_mod.shape[1]
    vectors = [ref[...].astype(f32) for ref in (cond_latent_ref, cond_context_ref)]
    vectors = [vector * (1.0 / (1.0 + jnp.exp(-vector))) for vector in vectors]
    lane_rows = depth // HEAD
    for j in range(lane_rows):
        pair = [vector[j : j + 1, :] for vector in vectors]
        act_ref[0:2, j * HEAD : (j + 1) * HEAD] = jnp.concatenate(pair, axis=0)
    mine_at = pl.ds(pl.multiple_of(sp * mod_rows, 128), mod_rows)
    act = act_ref[:, mine_at]
    act_row = lax.broadcasted_iota(jnp.int32, act.shape, 0)
    act = jnp.where(act_row < 2, act, 0.0).astype(bf16)
    for which, name in enumerate(("shift", "scale")):
        loads[name].wait()
        got = jnp.dot(act, w_mod[which], preferred_element_type=f32)
        part[2 * which : 2 * which + 2, :] = got[0:2, :]
    pl.semaphore_wait(barrier, n_grp + n_sp + n_tp - 3)

    def mod_copy(k):
        return pltpu.make_async_remote_copy(
            src_ref=part,
            dst_ref=part_in.at[k - 1],
            send_sem=mod_send.at[k - 1],
            recv_sem=mod_recv.at[k - 1],
            device_id={"sp": lax.rem(sp + k, n_sp)},
            device_id_type=MESH,
        )

    for k in range(1, n_sp):
        mod_copy(k).start()
    load("gate", 2, w_gate_hbm, w_mod.at[2])
    load("key", 5, w_key_hbm, w_key)
    load("value", 6, w_value_hbm, w_value)
    load("query", 7, w_query_hbm, w_query)
    load("out", 8, w_out_hbm.at[:, pl.ds(0, shared)], w_all.at[tp])
    load("rest", 9, w_out_hbm.at[:, pl.ds(shared, depth - shared)], w_rest)

    def columns_of(group, i):
        return pl.ds(pl.multiple_of((i * n_grp + group) * share, 128), share)

    def source(k, which):
        return lax.rem(chip - k + chips, chips) * 2 + which

    def beside_own():
        return pltpu.make_async_remote_copy(
            src_ref=w_out_hbm.at[:, pl.ds(0, shared)],
            dst_ref=w_all.at[tp],
            send_sem=own_send.at[0],
            recv_sem=own_recv.at[0],
            device_id={"tp": partner},
            device_id_type=MESH,
        )

    def across(k, i):
        cols = columns_of(grp, i)
        return pltpu.make_async_remote_copy(
            src_ref=w_out_hbm.at[:, cols],
            dst_ref=w_all.at[tp, :, cols],
            send_sem=across_send.at[k - 1, i],
            recv_sem=across_recv.at[k - 1, i],
            device_id={"tp": lax.rem(chip + k, chips) * 2 + core},
            device_id_type=MESH,
        )

    def relay(held, send, recv, to):
        return pltpu.make_async_remote_copy(
            src_ref=held,
            dst_ref=held,
            send_sem=send,
            recv_sem=recv,
            device_id=to,
            device_id_type=MESH,
        )

    def beside(k, i, which=None):
        which = core if which is None else which
        held = w_all.at[source(k, which), :, columns_of(grp, i)]
        return relay(
            held, beside_send.at[k - 1, i], beside_recv.at[k - 1, i], {"tp": partner}
        )

    def over(j, k, i, group=None):
        group = grp if group is None else group
        held = w_all.at[source(k, core), :, columns_of(group, i)]
        return relay(
            held,
            over_send.at[j - 1, k - 1, i],
            over_recv.at[j - 1, k - 1, i],
            {"grp": lax.rem(grp + j, n_grp)},
        )

    def last(j, k, i, which=None):
        which = core if which is None else which
        group = lax.rem(grp - j + n_grp, n_grp)
        held = w_all.at[source(k, which), :, columns_of(group, i)]
        return relay(
            held,
            last_send.at[j - 1, k - 1, i],
            last_recv.at[j - 1, k - 1, i],
            {"tp": partner},
        )

    def pass_on(i):
        for k in range(1, chips):
            across(k, i).wait_recv()
            for j in range(1, n_grp):
                over(j, k, i).start()
            beside(k, i).start()

    def pass_over(i):
        for j in range(1, n_grp):
            for k in range(1, chips):
                over(j, k, i, lax.rem(grp - j + n_grp, n_grp)).wait_recv()
                last(j, k, i).start()


    loads["latent"].wait()
    loads["context"].wait()

    def stats(i, carry):
        at = pl.ds(pl.multiple_of(i * 16, 16), 16)
        piece = x[at, :].astype(f32)
        inv[at, :] = lax.rsqrt(jnp.mean(piece * piece, axis=-1, keepdims=True) + epsilon)
        return carry

    lax.fori_loop(0, rows // 16, stats, 0, unroll=2)

    for k in range(1, n_sp):
        mod_copy(k).wait_recv()
    whole = part[...]
    for k in range(1, n_sp):
        whole = whole + part_in[k - 1]
    summed[...] = whole
    mod[tp] = whole

    def mod2_copy(k):
        return pltpu.make_async_remote_copy(
            src_ref=summed,
            dst_ref=mod.at[tp],
            send_sem=mod2_send.at[k - 1],
            recv_sem=mod2_recv.at[k - 1],
            device_id={"tp": lax.rem(tp + k, n_tp)},
            device_id_type=MESH,
        )

    for k in range(1, n_tp):
        mod2_copy(k).start()
    beside_own().start()
    for i in range(turns):
        for k in range(1, chips):
            across(k, i).start()

    def gate_copy(k):
        return pltpu.make_async_remote_copy(
            src_ref=gate_part,
            dst_ref=gate_in.at[k - 1],
            send_sem=gate_send.at[k - 1],
            recv_sem=gate_recv.at[k - 1],
            device_id={"sp": lax.rem(sp + k, n_sp)},
            device_id_type=MESH,
        )

    def gate2_copy(k):
        return pltpu.make_async_remote_copy(
            src_ref=gate_sum,
            dst_ref=gate_mod.at[tp],
            send_sem=gate2_send.at[k - 1],
            recv_sem=gate2_recv.at[k - 1],
            device_id={"tp": lax.rem(tp + k, n_tp)},
            device_id_type=MESH,
        )

    loads["gate"].wait()
    gate_part[...] = jnp.dot(act, w_mod[2], preferred_element_type=f32)[0:2, :]
    for k in range(1, n_sp):
        gate_copy(k).start()
    for k in range(1, n_tp):
        mod2_copy(k).wait_recv()

    def normalize(low, high):
        for start in range(low, high, 16):
            row = 0 if start < tok else 1
            at = slice(start, start + 16)
            for j in range(n_tp):
                cols = slice(j * mod_cols, (j + 1) * mod_cols)
                factor = gain_ref[:, cols] * (1.0 + mod[j, 2 + row : 3 + row, :])
                shift = mod[j, row : row + 1, :]
                piece = x[at, cols].astype(f32)
                x[at, cols] = (piece * inv[at, :] * factor + shift).astype(bf16)

    def turn(vector, gain, at):
        vector = vector * lax.rsqrt(jnp.mean(vector * vector, axis=-1, keepdims=True) + epsilon) * gain
        ahead = pltpu.roll(vector, HEAD - HEAD // 4, 1)
        behind = pltpu.roll(vector, HEAD // 4, 1)
        return vector * cos_ref[at, :] + ahead * sin_a_ref[at, :] + behind * sin_b_ref[at, :]

    def stream_copy(block, step, c, send, recv, to):
        held = kv.at[block, pl.ds(pl.multiple_of(c * kv_tile, 16), kv_tile)]
        return pltpu.make_async_remote_copy(
            src_ref=held,
            dst_ref=held,
            send_sem=send.at[step, c],
            recv_sem=recv.at[step, c],
            device_id={"sp": to},
            device_id_type=MESH,
        )

    to_right = jnp.minimum(sp + 1, n_sp - 1)
    to_left = jnp.maximum(sp - 1, 0)

    def right_copy(step, c):
        return stream_copy(jnp.maximum(sp - step, 0), step, c, right_send, right_recv, to_right)

    def left_copy(step, c):
        return stream_copy(jnp.minimum(sp + step, n_sp - 1), step, c, left_send, left_recv, to_left)

    def right_arrival(step, c):
        return stream_copy(jnp.maximum(sp - 1 - step, 0), step, c, right_send, right_recv, to_right)

    def left_arrival(step, c):
        return stream_copy(
            jnp.minimum(sp + 1 + step, n_sp - 1), step, c, left_send, left_recv, to_left
        )

    for c in range(kv_chunks):
        low, high = c * kv_tile, (c + 1) * kv_tile
        at = slice(low, high)
        normalize(low, high)
        if c == 0:
            loads["key"].wait()
            loads["value"].wait()
        raw = jnp.dot(x[at, :], w_key[...], preferred_element_type=f32)
        raw_values = jnp.dot(x[at, :], w_value[...], preferred_element_type=f32)
        for h in range(kv_heads):
            cols = slice(h * HEAD, (h + 1) * HEAD)
            kv[sp, at, cols] = turn(raw[:, cols], k_gain_ref[...], at).astype(bf16)
        kv[sp, at, kv_cols:] = raw_values.astype(bf16)

        @pl.when(sp < n_sp - 1)
        def _():
            right_copy(0, c).start()

        @pl.when(sp > 0)
        def _():
            left_copy(0, c).start()

    q_tile = tile_of(tok, 256)

    def project_queries(i, carry):
        at = pl.ds(pl.multiple_of(i * q_tile, 16), q_tile)
        raw = jnp.dot(x[at, :], w_query[...], preferred_element_type=f32)
        for h in range(heads):
            cols = slice(h * HEAD, (h + 1) * HEAD)
            queries[at, cols] = turn(raw[:, cols], q_gain_ref[...], at).astype(bf16)
        return carry

    stream = (n_sp - 1) * kv_chunks

    def serve(j):
        step = j // kv_chunks
        c = lax.rem(j, kv_chunks)

        @pl.when(jnp.logical_and(j < stream, jnp.logical_and(sp - 1 - step >= 0, sp < n_sp - 1)))
        def _():
            right_arrival(step, c).wait_recv()
            right_copy(step + 1, c).start()

        @pl.when(jnp.logical_and(j < stream, jnp.logical_and(sp + 1 + step <= n_sp - 1, sp > 0)))
        def _():
            left_arrival(step, c).wait_recv()
            left_copy(step + 1, c).start()

    loads["query"].wait()
    q_steps = tok // q_tile
    for i in range(q_steps):
        project_queries(i, 0)
        if i == max(q_steps - 2, 0):
            serve(jnp.int32(0))
    serve(jnp.int32(1))

    scaling = HEAD ** (-0.5)
    a_tile = tile_of(tok, 128)

    def attend(block, unit, first):
        held = pl.ds(pl.multiple_of(unit * unit_rows, 16), unit_rows)
        lane = unit * unit_rows + lax.broadcasted_iota(jnp.int32, (1, unit_rows), 1)
        lift = jnp.where(lane >= tok, context_lift, 0.0).astype(f32)
        spans = [slice(h * HEAD, (h + 1) * HEAD) for h in range(heads)]

        def one(i, carry):
            at = pl.ds(pl.multiple_of(i * a_tile, 16), a_tile)
            scores = []
            for h in range(heads):
                kv_span = slice((h // GROUP) * HEAD, (h // GROUP + 1) * HEAD)
                scores.append(
                    lax.dot_general(
                        queries[at, spans[h]],
                        kv[block, held, kv_span],
                        (((1,), (1,)), ((), ())),
                        preferred_element_type=f32,
                    )
                    * scaling
                    + lift
                )
            highs, fades, sums, products = [], [], [], []
            for h in range(heads):
                high = jnp.max(scores[h], axis=-1, keepdims=True)
                if not first:
                    old = top[h, at, :]
                    high = jnp.maximum(high, old)
                    fades.append(jnp.exp(old - high))
                highs.append(high)
                weights = jnp.exp(scores[h] - high)
                sums.append(jnp.sum(weights, axis=-1, keepdims=True))
                begin = kv_cols + (h // GROUP) * HEAD
                products.append(
                    jnp.dot(
                        weights.astype(bf16),
                        kv[block, held, begin : begin + HEAD],
                        preferred_element_type=f32,
                    )
                )
            if not first:
                sums = [total[h, at, :] * fades[h] + sums[h] for h in range(heads)]
                products = [acc[at, spans[h]] * fades[h] + products[h] for h in range(heads)]
            for h in range(heads):
                top[h, at, :] = highs[h]
                total[h, at, :] = sums[h]
                acc[at, spans[h]] = products[h]
            return carry

        lax.fori_loop(0, tok // a_tile, one, 0)

    early = min(2, turns)
    for i in range(early):
        pass_on(i)
    attend(sp, 0, True)
    serve(jnp.int32(2))
    for unit in range(1, units):
        attend(sp, unit, False)
    serve(jnp.int32(3))
    ahead = 4

    for k in range(1, n_sp):
        gate_copy(k).wait_recv()
    gate_whole = gate_part[...]
    for k in range(1, n_sp):
        gate_whole = gate_whole + gate_in[k - 1]
    gate_sum[...] = gate_whole
    gate_mod[tp] = gate_whole
    for k in range(1, n_tp):
        gate2_copy(k).start()
    if turns > early:
        pass_on(early)

    steps = (n_sp - 1) * units
    events = {}
    for i in range(early + 1, turns):
        events.setdefault(min(2 * (i - early - 1), steps), []).append((pass_on, i))
    for i in range(turns):
        at = i if i < 4 else i + 1
        if i == turns - 1:
            at = steps
        events.setdefault(min(at, steps), []).append((pass_over, i))

    def gather_step(t, carry):
        step = t // units
        unit = lax.rem(t, units)
        from_left = sp - 1 - step >= 0
        from_right = sp + 1 + step <= n_sp - 1
        per = per_unit
        for k in range((per + 1) // 2):
            serve(ahead + t * per + k)

        @pl.when(from_left)
        def _():
            @pl.when(sp == n_sp - 1)
            def _():
                for k in range(per):
                    right_arrival(step, unit * per + k).wait_recv()

            attend(jnp.maximum(sp - 1 - step, 0), unit, False)

        for k in range((per + 1) // 2, per):
            serve(ahead + t * per + k)

        @pl.when(from_right)
        def _():
            @pl.when(sp == 0)
            def _():
                for k in range(per):
                    left_arrival(step, unit * per + k).wait_recv()

            attend(jnp.minimum(sp + 1 + step, n_sp - 1), unit, False)

        for at in sorted(events):
            if at < steps:

                @pl.when(t == at)
                def _():
                    for act_on, i in events[at]:
                        act_on(i)

        return carry

    lax.fori_loop(0, steps, gather_step, 0)

    def finish(i, carry):
        at = pl.ds(pl.multiple_of(i * a_tile, 16), a_tile)
        for h in range(heads):
            cols = slice(h * HEAD, (h + 1) * HEAD)
            attended[at, cols] = (acc[at, cols] / total[h, at, :]).astype(bf16)
        return carry

    lax.fori_loop(0, tok // a_tile, finish, 0)

    def att_copy(k):
        to = lax.rem(tp + k, n_tp)
        return pltpu.make_async_remote_copy(
            src_ref=attended.at[pl.ds(pl.multiple_of(to * piece, 16), piece)],
            dst_ref=att_all.at[tp],
            send_sem=att_send.at[k - 1],
            recv_sem=att_recv.at[k - 1],
            device_id={"tp": to},
            device_id_type=MESH,
        )

    for k in range(1, n_tp):
        att_copy(k).start()
    att_all[tp] = attended[pl.ds(pl.multiple_of(tp * piece, 16), piece), :]
    for act_on, i in events.get(steps, []):
        act_on(i)
    width = pair_out.shape[3]
    chunks = pair_out.shape[1]

    def pair_copy(k, c):
        return pltpu.make_async_remote_copy(
            src_ref=pair_out.at[k, c],
            dst_ref=pair_in.at[k, c],
            send_sem=pair_send.at[k, c],
            recv_sem=pair_recv.at[k, c],
            device_id={"tp": partner},
            device_id_type=MESH,
        )

    def far_copy(k, c):
        return pltpu.make_async_remote_copy(
            src_ref=far_out.at[k - 1, c],
            dst_ref=far_in.at[k - 1, c],
            send_sem=far_send.at[k - 1, c],
            recv_sem=far_recv.at[k - 1, c],
            device_id={"tp": lax.rem(chip + k, chips) * 2 + core},
            device_id_type=MESH,
        )

    def multiply(k, c):
        to = lax.rem(chip + k, chips)
        cols = pl.ds(pl.multiple_of(c * width, width), width)

        def part_of(which):
            at = pl.ds(pl.multiple_of((to * 2 + which) * piece, 16), piece)
            return jnp.dot(
                attended[at, :], w_rest[:, cols], preferred_element_type=f32
            ).astype(bf16)

        pair_out[k, c] = part_of(1 - core)
        pair_copy(k, c).start()
        mine[k, c] = part_of(core)

    def combine(k, c):
        pair_copy(k, c).wait_recv()
        far_out[k - 1, c] = (mine[k, c].astype(f32) + pair_in[k, c].astype(f32)).astype(bf16)
        far_copy(k, c).start()

    loads["rest"].wait()
    for k in range(1, chips):
        for c in range(chunks):
            multiply(k, c)
        for c in range(chunks):
            combine(k, c)
    for c in range(chunks):
        multiply(0, c)

    def product(source_at, cols):
        return (
            jnp.dot(att_all[source_at], w_all[source_at, :, cols], preferred_element_type=f32)
            .astype(bf16)
            .astype(f32)
        )

    loads["out"].wait()
    beside_own().wait_recv()
    for k in range(1, n_tp):
        att_copy(k).wait_recv()
    blocks = shared // width
    for c in range(blocks):
        cols = slice(c * width, (c + 1) * width)
        acc_out[:, cols] = product(tp, cols) + product(partner, cols)

    for i in range(turns):
        for k in range(1, chips):
            beside(k, i, 1 - core).wait_recv()
            for j in range(1, n_grp):
                last(j, k, i, 1 - core).wait_recv()
    for k in range(1, n_tp):
        gate2_copy(k).wait_recv()
    per = mod_cols // width
    for c in range(blocks):
        cols = slice(c * width, (c + 1) * width)
        result = acc_out[:, cols]
        for k in range(1, chips):
            for which in range(2):
                result = result + product(source(k, which), cols)
        first = (c % per) * width
        gate = gate_mod[c // per, 0:1, first : first + width]
        out_ref[:, cols] = (gate * result).astype(bf16)
    for c in range(chunks):
        pair_copy(0, c).wait_recv()
        result = mine[0, c].astype(f32) + pair_in[0, c].astype(f32)
        for k in range(1, chips):
            far_copy(k, c).wait_recv()
            result = result + far_in[k - 1, c].astype(f32)
        at = blocks + c
        first = (at % per) * width
        gate = gate_mod[at // per, 0:1, first : first + width]
        out_ref[:, at * width : (at + 1) * width] = (gate * result).astype(bf16)

    beside_own().wait_send()
    for k in range(1, n_tp):
        att_copy(k).wait_send()
    for k in range(1, chips):
        for i in range(turns):
            across(k, i).wait_send()
            beside(k, i).wait_send()
            for j in range(1, n_grp):
                over(j, k, i).wait_send()
                last(j, k, i).wait_send()
    for k in range(1, n_sp):
        mod_copy(k).wait_send()
        gate_copy(k).wait_send()
    for k in range(1, n_tp):
        mod2_copy(k).wait_send()
        gate2_copy(k).wait_send()

    def drain(step, carry):
        for which in range(kv_chunks):

            @pl.when(jnp.logical_and(sp < n_sp - 1, sp - step >= 0))
            def _():
                right_copy(step, which).wait_send()

            @pl.when(jnp.logical_and(sp > 0, sp + step <= n_sp - 1))
            def _():
                left_copy(step, which).wait_send()

        return carry

    lax.fori_loop(0, n_sp - 1, drain, 0)
    for c in range(chunks):
        pair_copy(0, c).wait_send()
        for k in range(1, chips):
            pair_copy(k, c).wait_send()
            far_copy(k, c).wait_send()


def body(
    n_grp,
    n_sp,
    n_tp,
    latent,
    context,
    cond_latent,
    cond_context,
    w_shift,
    w_scale,
    w_gate,
    norm_gain,
    w_query,
    w_key,
    w_value,
    q_gain,
    k_gain,
    w_out,
):
    tok, depth = latent.shape
    ctx = context.shape[0]
    rows = tok + ctx
    mod_rows, mod_cols = w_shift.shape
    chips = n_tp // 2
    piece = tok // n_tp
    width = min(512, mod_cols)
    share = min(256, width)
    turns = (3 * depth // 4) // (n_grp * share)
    shared = turns * n_grp * share
    shared -= shared % width
    turns = shared // (n_grp * share)
    chunks = (depth - shared) // width
    kv_cols = w_key.shape[1]
    q_cols = w_query.shape[1]
    heads = q_cols // HEAD
    vmem = pl.BlockSpec(memory_space=pltpu.VMEM)
    hbm = pl.BlockSpec(memory_space=pl.ANY)
    dma = pltpu.SemaphoreType.DMA
    far = max(chips - 1, 1)
    others = max(n_grp - 1, 1)
    kv_chunks = rows // tile_of(rows, 128)
    return pl.pallas_call(
        functools.partial(kernel, n_grp, n_sp, n_tp, tok, ctx, share),
        out_shape=jax.ShapeDtypeStruct((piece, depth), bf16),
        in_specs=[vmem] * 5 + [hbm] * 9,
        out_specs=vmem,
        scratch_shapes=[
            pltpu.VMEM((16, depth), f32),
            pltpu.VMEM((rows, depth), bf16),
            pltpu.VMEM((3, mod_rows, mod_cols), bf16),
            pltpu.VMEM(w_query.shape, bf16),
            pltpu.VMEM(w_key.shape, bf16),
            pltpu.VMEM(w_value.shape, bf16),
            pltpu.VMEM((n_tp, w_out.shape[0], shared), bf16),
            pltpu.VMEM((w_out.shape[0], depth - shared), bf16),
            pltpu.VMEM((rows, 1), f32),
            pltpu.VMEM((rows, HEAD), f32),
            pltpu.VMEM((rows, HEAD), f32),
            pltpu.VMEM((rows, HEAD), f32),
            pltpu.VMEM((4, mod_cols), f32),
            pltpu.VMEM((n_sp - 1, 4, mod_cols), f32),
            pltpu.VMEM((4, mod_cols), f32),
            pltpu.VMEM((n_tp, 4, mod_cols), f32),
            pltpu.VMEM((2, mod_cols), f32),
            pltpu.VMEM((n_sp - 1, 2, mod_cols), f32),
            pltpu.VMEM((2, mod_cols), f32),
            pltpu.VMEM((n_tp, 2, mod_cols), f32),
            pltpu.VMEM((tok, q_cols), bf16),
            pltpu.VMEM((n_sp, rows, 2 * kv_cols), bf16),
            pltpu.VMEM((heads, tok, 1), f32),
            pltpu.VMEM((heads, tok, 1), f32),
            pltpu.VMEM((tok, q_cols), f32),
            pltpu.VMEM((tok, q_cols), bf16),
            pltpu.VMEM((n_tp, piece, q_cols), bf16),
            pltpu.VMEM((piece, shared), f32),
            pltpu.VMEM((chips, chunks, piece, width), bf16),
            pltpu.VMEM((chips, chunks, piece, width), bf16),
            pltpu.VMEM((chips, chunks, piece, width), bf16),
            pltpu.VMEM((far, chunks, piece, width), bf16),
            pltpu.VMEM((far, chunks, piece, width), bf16),
            dma((10,)),
            dma((n_sp - 1,)),
            dma((n_sp - 1,)),
            dma((n_tp - 1,)),
            dma((n_tp - 1,)),
            dma((n_sp - 1,)),
            dma((n_sp - 1,)),
            dma((n_tp - 1,)),
            dma((n_tp - 1,)),
            dma((n_sp, kv_chunks)),
            dma((n_sp, kv_chunks)),
            dma((n_sp, kv_chunks)),
            dma((n_sp, kv_chunks)),
            dma((chips, chunks)),
            dma((chips, chunks)),
            dma((far, chunks)),
            dma((far, chunks)),
            dma((1,)),
            dma((1,)),
            dma((far, turns)),
            dma((far, turns)),
            dma((far, turns)),
            dma((far, turns)),
            dma((others, far, turns)),
            dma((others, far, turns)),
            dma((others, far, turns)),
            dma((others, far, turns)),
            dma((n_tp - 1,)),
            dma((n_tp - 1,)),
        ],
        compiler_params=pltpu.CompilerParams(
            collective_id=0, has_side_effects=True, vmem_limit_bytes=60 * 1024 * 1024
        ),
    )(
        cond_latent.reshape(depth // HEAD, HEAD),
        cond_context.reshape(depth // HEAD, HEAD),
        norm_gain.reshape(1, depth),
        q_gain.reshape(1, HEAD),
        k_gain.reshape(1, HEAD),
        latent,
        context,
        w_shift,
        w_scale,
        w_gate,
        w_query,
        w_key,
        w_value,
        w_out,
    )


def solution(mesh):
    placed = (
        P(("grp", "sp"), None),
        P(("grp", "sp"), None),
        P("grp"),
        P(),
        P("sp", "tp"),
        P("sp", "tp"),
        P("sp", "tp"),
        P(),
        P(None, "tp"),
        P(None, "tp"),
        P(None, "tp"),
        P(),
        P(),
        P("tp", None),
    )
    return jax.shard_map(
        functools.partial(body, mesh.shape["grp"], mesh.shape["sp"], mesh.shape["tp"]),
        mesh=mesh,
        in_specs=placed,
        out_specs=P(("grp", "sp", "tp"), None),
        check_vma=False,
    )
```

```python
import functools
import math

import jax
import jax.numpy as jnp
from jax import lax
from jax.experimental import pallas as pl
from jax.experimental.pallas import tpu as pltpu
from jax.sharding import PartitionSpec as P

HEADS = 16
KV_HEADS = 8
HEAD = 128
GRID_W = 64
GROUP = HEADS // KV_HEADS

epsilon = 1e-06
context_lift = 1.5
rope_theta = 10000.0

MESH = pl.DeviceIdType.MESH
f32 = jnp.float32
bf16 = jnp.bfloat16


def tile_of(rows, most):
    best = 16
    for size in range(16, most + 1, 16):
        if rows % size == 0:
            best = size
    return best


def kernel(
    n_grp,
    n_sp,
    n_tp,
    tok,
    ctx,
    share,
    cond_latent_hbm,
    cond_context_hbm,
    gain_hbm,
    q_gain_hbm,
    k_gain_hbm,
    latent_hbm,
    context_hbm,
    w_shift_hbm,
    w_scale_hbm,
    w_gate_hbm,
    w_query_hbm,
    w_key_hbm,
    w_value_hbm,
    w_out_hbm,
    out_hbm,
    cond_latent_ref,
    cond_context_ref,
    gain_ref,
    q_gain_ref,
    k_gain_ref,
    out_ref,
    act_ref,
    x,
    w_mod,
    w_query,
    w_key,
    w_value,
    w_all,
    w_rest,
    inv,
    cos_ref,
    sin_a_ref,
    sin_b_ref,
    part,
    part_in,
    summed,
    mod,
    gate_part,
    gate_in,
    gate_sum,
    gate_mod,
    queries,
    kv,
    top,
    total,
    acc,
    attended,
    att_all,
    acc_out,
    pair_out,
    pair_in,
    mine,
    far_out,
    far_in,
    load_sem,
    mod_send,
    mod_recv,
    mod2_send,
    mod2_recv,
    gate_send,
    gate_recv,
    gate2_send,
    gate2_recv,
    right_send,
    right_recv,
    left_send,
    left_recv,
    pair_send,
    pair_recv,
    far_send,
    far_recv,
    own_send,
    own_recv,
    across_send,
    across_recv,
    beside_send,
    beside_recv,
    over_send,
    over_recv,
    last_send,
    last_recv,
    att_send,
    att_recv,
    out_sem,
):
    grp = lax.axis_index("grp")
    sp = lax.axis_index("sp")
    tp = lax.axis_index("tp")
    chips = n_tp // 2
    chip = tp // 2
    core = lax.rem(tp, 2)
    partner = chip * 2 + 1 - core
    piece = tok // n_tp
    turns = w_all.shape[2] // (n_grp * share)
    shared = w_all.shape[2]
    mod_rows = w_mod.shape[1]
    rows = tok + ctx
    depth = x.shape[1]
    mod_cols = mod.shape[2]
    heads = queries.shape[1] // HEAD
    kv_cols = kv.shape[2] // 2
    kv_heads = kv_cols // HEAD
    kv_tile = tile_of(rows, 128)
    kv_chunks = rows // kv_tile
    per_unit = 2 if kv_chunks % 2 == 0 else 1
    units = kv_chunks // per_unit
    unit_rows = kv_tile * per_unit

    loads = {}

    def load(name, index, source, target):
        loads[name] = pltpu.make_async_copy(source, target, load_sem.at[index])
        loads[name].start()

    load("cond_latent", 10, cond_latent_hbm, cond_latent_ref)
    load("cond_context", 11, cond_context_hbm, cond_context_ref)
    load("shift", 0, w_shift_hbm, w_mod.at[0])
    load("scale", 1, w_scale_hbm, w_mod.at[1])
    load("latent", 3, latent_hbm, x.at[pl.ds(0, tok)])
    load("context", 4, context_hbm, x.at[pl.ds(tok, ctx)])
    load("gain", 12, gain_hbm, gain_ref)
    load("q_gain", 13, q_gain_hbm, q_gain_ref)
    load("k_gain", 14, k_gain_hbm, k_gain_ref)

    barrier = pltpu.get_barrier_semaphore()
    for k in range(1, n_sp):
        pl.semaphore_signal(
            barrier, inc=1, device_id={"sp": lax.rem(sp + k, n_sp)}, device_id_type=MESH
        )
    for k in range(1, n_tp):
        pl.semaphore_signal(
            barrier, inc=1, device_id={"tp": lax.rem(tp + k, n_tp)}, device_id_type=MESH
        )

    for k in range(1, n_grp):
        pl.semaphore_signal(
            barrier, inc=1, device_id={"grp": lax.rem(grp + k, n_grp)}, device_id_type=MESH
        )

    loads["cond_latent"].wait()
    loads["cond_context"].wait()
    vectors = [ref[...].astype(f32) for ref in (cond_latent_ref, cond_context_ref)]
    vectors = [vector * (1.0 / (1.0 + jnp.exp(-vector))) for vector in vectors]
    lane_rows = depth // HEAD
    for j in range(lane_rows):
        pair = [vector[j : j + 1, :] for vector in vectors]
        act_ref[0:2, j * HEAD : (j + 1) * HEAD] = jnp.concatenate(pair, axis=0)
    mine_at = pl.ds(pl.multiple_of(sp * mod_rows, 128), mod_rows)
    act = act_ref[:, mine_at]
    act_row = lax.broadcasted_iota(jnp.int32, act.shape, 0)
    act = jnp.where(act_row < 2, act, 0.0).astype(bf16)
    for which, name in enumerate(("shift", "scale")):
        loads[name].wait()
        got = jnp.dot(act, w_mod[which], preferred_element_type=f32)
        part[2 * which : 2 * which + 2, :] = got[0:2, :]
    pl.semaphore_wait(barrier, n_grp + n_sp + n_tp - 3)

    def all_of(held, send, recv):
        return pltpu.make_async_remote_copy(
            src_ref=held,
            dst_ref=held,
            send_sem=send,
            recv_sem=recv,
            device_id={"tp": partner},
            device_id_type=MESH,
        )

    def mod_copy(k):
        return pltpu.make_async_remote_copy(
            src_ref=part,
            dst_ref=part_in.at[k - 1],
            send_sem=mod_send.at[0],
            recv_sem=mod_recv.at[0],
            device_id={"sp": lax.rem(sp + k, n_sp)},
            device_id_type=MESH,
        )

    for k in range(1, n_sp):
        mod_copy(k).start()
    load("gate", 2, w_gate_hbm, w_mod.at[2])
    load("key", 5, w_key_hbm, w_key)
    load("value", 6, w_value_hbm, w_value)
    load("query", 7, w_query_hbm, w_query)
    load("out", 8, w_out_hbm.at[:, pl.ds(0, shared)], w_all.at[tp])
    load("rest", 9, w_out_hbm.at[:, pl.ds(shared, depth - shared)], w_rest)

    def columns_of(group, i):
        return pl.ds(pl.multiple_of((i * n_grp + group) * share, 128), share)

    def source(k, which):
        return lax.rem(chip - k + chips, chips) * 2 + which

    def beside_own():
        return pltpu.make_async_remote_copy(
            src_ref=w_out_hbm.at[:, pl.ds(0, shared)],
            dst_ref=w_all.at[tp],
            send_sem=own_send.at[0],
            recv_sem=own_recv.at[0],
            device_id={"tp": partner},
            device_id_type=MESH,
        )

    def across(k, i):
        cols = columns_of(grp, i)
        return pltpu.make_async_remote_copy(
            src_ref=w_out_hbm.at[:, cols],
            dst_ref=w_all.at[tp, :, cols],
            send_sem=across_send.at[0],
            recv_sem=across_recv.at[k - 1, i],
            device_id={"tp": lax.rem(chip + k, chips) * 2 + core},
            device_id_type=MESH,
        )

    def relay(held, send, recv, to):
        return pltpu.make_async_remote_copy(
            src_ref=held,
            dst_ref=held,
            send_sem=send,
            recv_sem=recv,
            device_id=to,
            device_id_type=MESH,
        )

    in_block = pair_out.shape[3] // (n_grp * share)
    tail_from = turns - in_block

    def batch_of(i):
        return 0 if i < tail_from else 1

    def beside(k, i, which=None):
        which = core if which is None else which
        held = w_all.at[source(k, which), :, columns_of(grp, i)]
        return relay(
            held, beside_send.at[0], beside_recv.at[batch_of(i)], {"tp": partner}
        )

    def over(j, k, i, group=None):
        group = grp if group is None else group
        held = w_all.at[source(k, core), :, columns_of(group, i)]
        return relay(
            held,
            over_send.at[0],
            over_recv.at[j - 1, k - 1, i],
            {"grp": lax.rem(grp + j, n_grp)},
        )

    def last(j, k, i, which=None):
        which = core if which is None else which
        group = lax.rem(grp - j + n_grp, n_grp)
        held = w_all.at[source(k, which), :, columns_of(group, i)]
        return relay(
            held,
            last_send.at[0],
            last_recv.at[batch_of(i)],
            {"tp": partner},
        )

    def pass_on(i):
        for k in range(1, chips):
            across(k, i).wait_recv()
            for j in range(1, n_grp):
                over(j, k, i).start()
            beside(k, i).start()

    def pass_over(i):
        for j in range(1, n_grp):
            for k in range(1, chips):
                over(j, k, i, lax.rem(grp - j + n_grp, n_grp)).wait_recv()
                last(j, k, i).start()


    loads["latent"].wait()
    loads["context"].wait()

    def stats(i, carry):
        at = pl.ds(pl.multiple_of(i * 16, 16), 16)
        piece = x[at, :].astype(f32)
        inv[at, :] = lax.rsqrt(jnp.mean(piece * piece, axis=-1, keepdims=True) + epsilon)
        return carry

    lax.fori_loop(0, rows // 16, stats, 0, unroll=2)

    all_of(part_in, mod_send.at[0], mod_recv.at[0]).wait_recv()
    whole = part[...]
    for k in range(1, n_sp):
        whole = whole + part_in[k - 1]
    summed[...] = whole
    mod[tp] = whole

    def mod2_copy(k):
        return pltpu.make_async_remote_copy(
            src_ref=summed,
            dst_ref=mod.at[tp],
            send_sem=mod2_send.at[0],
            recv_sem=mod2_recv.at[0],
            device_id={"tp": lax.rem(tp + k, n_tp)},
            device_id_type=MESH,
        )

    for k in range(1, n_tp):
        mod2_copy(k).start()
    beside_own().start()
    for i in range(turns):
        for k in range(1, chips):
            across(k, i).start()

    def gate_copy(k):
        return pltpu.make_async_remote_copy(
            src_ref=gate_part,
            dst_ref=gate_in.at[k - 1],
            send_sem=gate_send.at[0],
            recv_sem=gate_recv.at[0],
            device_id={"sp": lax.rem(sp + k, n_sp)},
            device_id_type=MESH,
        )

    def gate2_copy(k):
        return pltpu.make_async_remote_copy(
            src_ref=gate_sum,
            dst_ref=gate_mod.at[tp],
            send_sem=gate2_send.at[0],
            recv_sem=gate2_recv.at[0],
            device_id={"tp": lax.rem(tp + k, n_tp)},
            device_id_type=MESH,
        )

    loads["gate"].wait()
    gate_part[...] = jnp.dot(act, w_mod[2], preferred_element_type=f32)[0:2, :]
    for k in range(1, n_sp):
        gate_copy(k).start()
    def tables(i, carry):
        at = pl.ds(pl.multiple_of(i * 16, 16), 16)
        index = i * 16 + lax.broadcasted_iota(jnp.int32, (16, HEAD), 0)
        lane = lax.broadcasted_iota(jnp.int32, (16, HEAD), 1)
        freqs = HEAD // 4
        position = sp * tok + index
        inverse = jnp.exp(lax.rem(lane, freqs).astype(f32) * (-math.log(rope_theta) / freqs))
        place = jnp.where(lane < 2 * freqs, lax.div(position, GRID_W), lax.rem(position, GRID_W))
        angle = jnp.where(index < tok, place.astype(f32) * inverse, 0.0)
        sine = jnp.sin(angle)
        first_half = lax.rem(lax.div(lane, freqs), 2) == 0
        cos_ref[at, :] = jnp.cos(angle)
        sin_a_ref[at, :] = jnp.where(first_half, -sine, 0.0)
        sin_b_ref[at, :] = jnp.where(first_half, 0.0, sine)
        return carry

    lax.fori_loop(0, rows // 16, tables, 0)
    all_of(mod.at[pl.ds(0, n_tp - 1)], mod2_send.at[0], mod2_recv.at[0]).wait_recv()
    for name in ("gain", "q_gain", "k_gain"):
        loads[name].wait()

    def normalize(low, high):
        for start in range(low, high, 16):
            row = 0 if start < tok else 1
            at = slice(start, start + 16)
            for j in range(n_tp):
                cols = slice(j * mod_cols, (j + 1) * mod_cols)
                factor = gain_ref[:, cols] * (1.0 + mod[j, 2 + row : 3 + row, :])
                shift = mod[j, row : row + 1, :]
                piece = x[at, cols].astype(f32)
                x[at, cols] = (piece * inv[at, :] * factor + shift).astype(bf16)

    def turn(vector, gain, at):
        vector = vector * lax.rsqrt(jnp.mean(vector * vector, axis=-1, keepdims=True) + epsilon) * gain
        ahead = pltpu.roll(vector, HEAD - HEAD // 4, 1)
        behind = pltpu.roll(vector, HEAD // 4, 1)
        return vector * cos_ref[at, :] + ahead * sin_a_ref[at, :] + behind * sin_b_ref[at, :]

    def stream_copy(block, step, c, send, recv, to):
        held = kv.at[block, pl.ds(pl.multiple_of(c * kv_tile, 16), kv_tile)]
        return pltpu.make_async_remote_copy(
            src_ref=held,
            dst_ref=held,
            send_sem=send.at[0],
            recv_sem=recv.at[step, c],
            device_id={"sp": to},
            device_id_type=MESH,
        )

    to_right = jnp.minimum(sp + 1, n_sp - 1)
    to_left = jnp.maximum(sp - 1, 0)

    def right_copy(step, c):
        return stream_copy(jnp.maximum(sp - step, 0), step, c, right_send, right_recv, to_right)

    def left_copy(step, c):
        return stream_copy(jnp.minimum(sp + step, n_sp - 1), step, c, left_send, left_recv, to_left)

    def right_arrival(step, c):
        return stream_copy(jnp.maximum(sp - 1 - step, 0), step, c, right_send, right_recv, to_right)

    def left_arrival(step, c):
        return stream_copy(
            jnp.minimum(sp + 1 + step, n_sp - 1), step, c, left_send, left_recv, to_left
        )

    def early_pass(act_on, i):
        if i < turns:
            act_on(i)

    for c in range(kv_chunks):
        low, high = c * kv_tile, (c + 1) * kv_tile
        at = slice(low, high)
        normalize(low, high)
        if c == 0:
            loads["key"].wait()
            loads["value"].wait()
        raw = jnp.dot(x[at, :], w_key[...], preferred_element_type=f32)
        raw_values = jnp.dot(x[at, :], w_value[...], preferred_element_type=f32)
        for h in range(kv_heads):
            cols = slice(h * HEAD, (h + 1) * HEAD)
            kv[sp, at, cols] = turn(raw[:, cols], k_gain_ref[...], at).astype(bf16)
        kv[sp, at, kv_cols:] = raw_values.astype(bf16)

        @pl.when(sp < n_sp - 1)
        def _():
            right_copy(0, c).start()

        @pl.when(sp > 0)
        def _():
            left_copy(0, c).start()

        if c == min(1, kv_chunks - 1):
            early_pass(pass_on, 0)

    early_pass(pass_on, 1)
    q_tile = tile_of(tok, 256)

    def project_queries(i, carry):
        at = pl.ds(pl.multiple_of(i * q_tile, 16), q_tile)
        raw = jnp.dot(x[at, :], w_query[...], preferred_element_type=f32)
        for h in range(heads):
            cols = slice(h * HEAD, (h + 1) * HEAD)
            queries[at, cols] = turn(raw[:, cols], q_gain_ref[...], at).astype(bf16)
        return carry

    stream = (n_sp - 1) * kv_chunks

    def serve(j):
        step = j // kv_chunks
        c = lax.rem(j, kv_chunks)

        @pl.when(jnp.logical_and(j < stream, jnp.logical_and(sp - 1 - step >= 0, sp < n_sp - 1)))
        def _():
            right_arrival(step, c).wait_recv()
            right_copy(step + 1, c).start()

        @pl.when(jnp.logical_and(j < stream, jnp.logical_and(sp + 1 + step <= n_sp - 1, sp > 0)))
        def _():
            left_arrival(step, c).wait_recv()
            left_copy(step + 1, c).start()

    loads["query"].wait()
    q_steps = tok // q_tile
    for i in range(q_steps):
        project_queries(i, 0)
        if i == max(q_steps - 2, 0):
            serve(jnp.int32(0))
    serve(jnp.int32(1))

    scaling = HEAD ** (-0.5)
    a_tile = tile_of(tok, 128)

    def attend(block, unit, first):
        held = pl.ds(pl.multiple_of(unit * unit_rows, 16), unit_rows)
        lane = unit * unit_rows + lax.broadcasted_iota(jnp.int32, (1, unit_rows), 1)
        lift = jnp.where(lane >= tok, context_lift, 0.0).astype(f32)
        spans = [slice(h * HEAD, (h + 1) * HEAD) for h in range(heads)]

        def one(i, carry):
            at = pl.ds(pl.multiple_of(i * a_tile, 16), a_tile)
            scores = []
            for h in range(heads):
                kv_span = slice((h // GROUP) * HEAD, (h // GROUP + 1) * HEAD)
                scores.append(
                    lax.dot_general(
                        queries[at, spans[h]],
                        kv[block, held, kv_span],
                        (((1,), (1,)), ((), ())),
                        preferred_element_type=f32,
                    )
                    * scaling
                    + lift
                )
            highs, fades, sums, products = [], [], [], []
            for h in range(heads):
                high = jnp.max(scores[h], axis=-1, keepdims=True)
                if not first:
                    old = top[h, at, :]
                    high = jnp.maximum(high, old)
                    fades.append(jnp.exp(old - high))
                highs.append(high)
                weights = jnp.exp(scores[h] - high)
                sums.append(jnp.sum(weights, axis=-1, keepdims=True))
                begin = kv_cols + (h // GROUP) * HEAD
                products.append(
                    jnp.dot(
                        weights.astype(bf16),
                        kv[block, held, begin : begin + HEAD],
                        preferred_element_type=f32,
                    )
                )
            if not first:
                sums = [total[h, at, :] * fades[h] + sums[h] for h in range(heads)]
                products = [acc[at, spans[h]] * fades[h] + products[h] for h in range(heads)]
            for h in range(heads):
                top[h, at, :] = highs[h]
                total[h, at, :] = sums[h]
                acc[at, spans[h]] = products[h]
            return carry

        lax.fori_loop(0, tok // a_tile, one, 0)

    early_pass(pass_on, 2)
    attend(sp, 0, True)
    early_pass(pass_over, 0)
    serve(jnp.int32(2))
    for unit in range(1, units):
        attend(sp, unit, False)
    serve(jnp.int32(3))
    ahead = 4
    early_pass(pass_on, 3)
    early_pass(pass_over, 1)

    all_of(gate_in, gate_send.at[0], gate_recv.at[0]).wait_recv()
    gate_whole = gate_part[...]
    for k in range(1, n_sp):
        gate_whole = gate_whole + gate_in[k - 1]
    gate_sum[...] = gate_whole
    gate_mod[tp] = gate_whole
    for k in range(1, n_tp):
        gate2_copy(k).start()
    steps = (n_sp - 1) * units
    events = {}
    halves = 2 * steps
    for i in range(4, turns):
        at = (0, 1, 2, 3, 5, 7, 9, 11)[i - 4] if i < 12 else i
        events.setdefault(min(at, halves - 1), []).append((pass_on, i))
    for i in range(2, turns):
        at = (1, 3, 4, 5, 6, 8, 10)[i - 2] if i < 9 else halves
        events.setdefault(min(at, halves), []).append((pass_over, i))

    def take_events(t, half):
        for at in sorted(events):
            if at < halves and at % 2 == half:

                @pl.when(t == at // 2)
                def _():
                    for act_on, i in events[at]:
                        act_on(i)

    def gather_step(t, carry):
        step = t // units
        unit = lax.rem(t, units)
        from_left = sp - 1 - step >= 0
        from_right = sp + 1 + step <= n_sp - 1
        per = per_unit
        for k in range((per + 1) // 2):
            serve(ahead + t * per + k)

        @pl.when(from_left)
        def _():
            @pl.when(sp == n_sp - 1)
            def _():
                for k in range(per):
                    right_arrival(step, unit * per + k).wait_recv()

            attend(jnp.maximum(sp - 1 - step, 0), unit, False)

        for k in range((per + 1) // 2, per):
            serve(ahead + t * per + k)

        take_events(t, 0)

        @pl.when(from_right)
        def _():
            @pl.when(sp == 0)
            def _():
                for k in range(per):
                    left_arrival(step, unit * per + k).wait_recv()

            attend(jnp.minimum(sp + 1 + step, n_sp - 1), unit, False)

        take_events(t, 1)
        return carry

    lax.fori_loop(0, steps, gather_step, 0)

    def att_copy(k):
        to = lax.rem(tp + k, n_tp)
        return pltpu.make_async_remote_copy(
            src_ref=attended.at[pl.ds(pl.multiple_of(to * piece, 16), piece)],
            dst_ref=att_all.at[tp],
            send_sem=att_send.at[0],
            recv_sem=att_recv.at[jnp.where(to == partner, 0, 1)],
            device_id={"tp": to},
            device_id_type=MESH,
        )

    def finish(k):
        at = pl.ds(pl.multiple_of(lax.rem(tp + k, n_tp) * piece, 16), piece)
        for h in range(heads):
            cols = slice(h * HEAD, (h + 1) * HEAD)
            attended[at, cols] = (acc[at, cols] / total[h, at, :]).astype(bf16)

    for k in range(2, n_tp + 2):
        finish(k)
        if k % n_tp:
            att_copy(k % n_tp).start()
    att_all[tp] = attended[pl.ds(pl.multiple_of(tp * piece, 16), piece), :]
    late = events.get(halves, [])
    width = pair_out.shape[3]
    chunks = pair_out.shape[1]

    def pair_copy(k, c):
        return pltpu.make_async_remote_copy(
            src_ref=pair_out.at[k, c],
            dst_ref=pair_in.at[k, c],
            send_sem=pair_send.at[0],
            recv_sem=pair_recv.at[k, c],
            device_id={"tp": partner},
            device_id_type=MESH,
        )

    def far_copy(k, c):
        return pltpu.make_async_remote_copy(
            src_ref=far_out.at[k - 1, c],
            dst_ref=far_in.at[k - 1, c],
            send_sem=far_send.at[0],
            recv_sem=far_recv.at[k - 1, c],
            device_id={"tp": lax.rem(chip + k, chips) * 2 + core},
            device_id_type=MESH,
        )

    def multiply(k, c):
        to = lax.rem(chip + k, chips)
        cols = pl.ds(pl.multiple_of(c * width, width), width)

        def part_of(which):
            at = pl.ds(pl.multiple_of((to * 2 + which) * piece, 16), piece)
            return jnp.dot(
                attended[at, :], w_rest[:, cols], preferred_element_type=f32
            ).astype(bf16)

        pair_out[k, c] = part_of(1 - core)
        pair_copy(k, c).start()
        mine[k, c] = part_of(core)

    def combine(k, c):
        pair_copy(k, c).wait_recv()
        far_out[k - 1, c] = (mine[k, c].astype(f32) + pair_in[k, c].astype(f32)).astype(bf16)
        far_copy(k, c).start()

    blocks = shared // width

    def product(source_at, cols):
        return (
            jnp.dot(att_all[source_at], w_all[source_at, :, cols], preferred_element_type=f32)
            .astype(bf16)
            .astype(f32)
        )

    loads["rest"].wait()
    loads["out"].wait()
    for k in range(1, chips):
        for c in range(chunks):
            multiply(k, c)
    for c in range(blocks):
        cols = slice(c * width, (c + 1) * width)
        acc_out[:, cols] = product(tp, cols)
    for k in range(1, chips):
        for c in range(chunks):
            combine(k, c)
    for c in range(chunks):
        multiply(0, c)
    beside_own().wait_recv()
    all_of(att_all.at[pl.ds(0, 1)], att_send.at[0], att_recv.at[0]).wait_recv()
    for c in range(blocks):
        cols = slice(c * width, (c + 1) * width)
        acc_out[:, cols] += product(partner, cols)
    for act_on, i in late:
        act_on(i)
    if chips > 1:
        all_of(att_all.at[pl.ds(0, n_tp - 2)], att_send.at[0], att_recv.at[1]).wait_recv()

    all_of(gate_mod.at[pl.ds(0, n_tp - 1)], gate2_send.at[0], gate2_recv.at[0]).wait_recv()
    per = mod_cols // width

    def put(at, result):
        cols = slice(at * width, (at + 1) * width)
        first = (at % per) * width
        gate = gate_mod[at // per, 0:1, first : first + width]
        out_ref[:, cols] = (gate * result).astype(bf16)
        out_copy(at).start()

    def out_copy(at):
        cols = pl.ds(at * width, width)
        return pltpu.make_async_copy(out_ref.at[:, cols], out_hbm.at[:, cols], out_sem.at[0])

    for c in range(blocks):
        if chips > 1 and c in (0, blocks - 1):
            batch = 0 if c == 0 and blocks > 1 else 1
            count = (tail_from if batch == 0 else in_block) * share
            for copies, sems in ((1, beside_recv), (n_grp - 1, last_recv)):
                if copies * count:
                    held = w_all.at[pl.ds(0, chips - 1), :, pl.ds(0, copies * count)]
                    all_of(held, own_send.at[0], sems.at[batch]).wait_recv()
        cols = slice(c * width, (c + 1) * width)
        result = acc_out[:, cols]
        for k in range(1, chips):
            for which in range(2):
                result = result + product(source(k, which), cols)
        put(c, result)
    for c in range(chunks):
        pair_copy(0, c).wait_recv()
        result = mine[0, c].astype(f32) + pair_in[0, c].astype(f32)
        for k in range(1, chips):
            far_copy(k, c).wait_recv()
            result = result + far_in[k - 1, c].astype(f32)
        put(blocks + c, result)

    beside_own().wait_send()
    all_of(att_all.at[pl.ds(0, n_tp - 1)], att_send.at[0], att_recv.at[0]).wait_send()
    if chips > 1:
        count = turns * share
        held = w_all.at[pl.ds(0, chips - 1), :, pl.ds(0, count)]
        all_of(held, across_send.at[0], own_recv.at[0]).wait_send()
        all_of(held, beside_send.at[0], own_recv.at[0]).wait_send()
        if n_grp > 1:
            held = w_all.at[pl.ds(0, chips - 1), :, pl.ds(0, (n_grp - 1) * count)]
            all_of(held, over_send.at[0], own_recv.at[0]).wait_send()
            all_of(held, last_send.at[0], own_recv.at[0]).wait_send()
    all_of(part_in, mod_send.at[0], mod_recv.at[0]).wait_send()
    all_of(gate_in, gate_send.at[0], gate_recv.at[0]).wait_send()
    all_of(mod.at[pl.ds(0, n_tp - 1)], mod2_send.at[0], mod2_recv.at[0]).wait_send()
    all_of(gate_mod.at[pl.ds(0, n_tp - 1)], gate2_send.at[0], gate2_recv.at[0]).wait_send()

    for at in range(n_sp):

        @pl.when(sp == at)
        def _():
            if at < n_sp - 1:
                all_of(kv.at[pl.ds(0, at + 1)], right_send.at[0], right_recv.at[0, 0]).wait_send()
            if at > 0:
                all_of(kv.at[pl.ds(0, n_sp - at)], left_send.at[0], left_recv.at[0, 0]).wait_send()

    all_of(pair_out, pair_send.at[0], pair_recv.at[0, 0]).wait_send()
    if chips > 1:
        all_of(far_out, far_send.at[0], far_recv.at[0, 0]).wait_send()
    pltpu.make_async_copy(out_ref, out_hbm, out_sem.at[0]).wait()


def body(
    n_grp,
    n_sp,
    n_tp,
    latent,
    context,
    cond_latent,
    cond_context,
    w_shift,
    w_scale,
    w_gate,
    norm_gain,
    w_query,
    w_key,
    w_value,
    q_gain,
    k_gain,
    w_out,
):
    tok, depth = latent.shape
    ctx = context.shape[0]
    rows = tok + ctx
    mod_rows, mod_cols = w_shift.shape
    chips = n_tp // 2
    piece = tok // n_tp
    width = min(512, mod_cols)
    share = min(128, width)
    turns = (3 * depth // 4) // (n_grp * share)
    shared = turns * n_grp * share
    shared -= shared % width
    turns = shared // (n_grp * share)
    chunks = (depth - shared) // width
    kv_cols = w_key.shape[1]
    q_cols = w_query.shape[1]
    heads = q_cols // HEAD
    hbm = pl.BlockSpec(memory_space=pl.ANY)
    dma = pltpu.SemaphoreType.DMA
    far = max(chips - 1, 1)
    others = max(n_grp - 1, 1)
    kv_chunks = rows // tile_of(rows, 128)
    return pl.pallas_call(
        functools.partial(kernel, n_grp, n_sp, n_tp, tok, ctx, share),
        out_shape=jax.ShapeDtypeStruct((piece, depth), bf16),
        in_specs=[hbm] * 14,
        out_specs=hbm,
        scratch_shapes=[
            pltpu.VMEM((depth // HEAD, HEAD), bf16),
            pltpu.VMEM((depth // HEAD, HEAD), bf16),
            pltpu.VMEM((1, depth), f32),
            pltpu.VMEM((1, HEAD), f32),
            pltpu.VMEM((1, HEAD), f32),
            pltpu.VMEM((piece, depth), bf16),
            pltpu.VMEM((16, depth), f32),
            pltpu.VMEM((rows, depth), bf16),
            pltpu.VMEM((3, mod_rows, mod_cols), bf16),
            pltpu.VMEM(w_query.shape, bf16),
            pltpu.VMEM(w_key.shape, bf16),
            pltpu.VMEM(w_value.shape, bf16),
            pltpu.VMEM((n_tp, w_out.shape[0], shared), bf16),
            pltpu.VMEM((w_out.shape[0], depth - shared), bf16),
            pltpu.VMEM((rows, 1), f32),
            pltpu.VMEM((rows, HEAD), f32),
            pltpu.VMEM((rows, HEAD), f32),
            pltpu.VMEM((rows, HEAD), f32),
            pltpu.VMEM((4, mod_cols), f32),
            pltpu.VMEM((n_sp - 1, 4, mod_cols), f32),
            pltpu.VMEM((4, mod_cols), f32),
            pltpu.VMEM((n_tp, 4, mod_cols), f32),
            pltpu.VMEM((2, mod_cols), f32),
            pltpu.VMEM((n_sp - 1, 2, mod_cols), f32),
            pltpu.VMEM((2, mod_cols), f32),
            pltpu.VMEM((n_tp, 2, mod_cols), f32),
            pltpu.VMEM((tok, q_cols), bf16),
            pltpu.VMEM((n_sp, rows, 2 * kv_cols), bf16),
            pltpu.VMEM((heads, tok, 1), f32),
            pltpu.VMEM((heads, tok, 1), f32),
            pltpu.VMEM((tok, q_cols), f32),
            pltpu.VMEM((tok, q_cols), bf16),
            pltpu.VMEM((n_tp, piece, q_cols), bf16),
            pltpu.VMEM((piece, shared), f32),
            pltpu.VMEM((chips, chunks, piece, width), bf16),
            pltpu.VMEM((chips, chunks, piece, width), bf16),
            pltpu.VMEM((chips, chunks, piece, width), bf16),
            pltpu.VMEM((far, chunks, piece, width), bf16),
            pltpu.VMEM((far, chunks, piece, width), bf16),
            dma((15,)),
            dma((1,)),
            dma((1,)),
            dma((1,)),
            dma((1,)),
            dma((1,)),
            dma((1,)),
            dma((1,)),
            dma((1,)),
            dma((1,)),
            dma((n_sp - 1, kv_chunks)),
            dma((1,)),
            dma((n_sp - 1, kv_chunks)),
            dma((1,)),
            dma((chips, chunks)),
            dma((1,)),
            dma((far, chunks)),
            dma((1,)),
            dma((1,)),
            dma((1,)),
            dma((far, turns)),
            dma((1,)),
            dma((2,)),
            dma((1,)),
            dma((others, far, turns)),
            dma((1,)),
            dma((2,)),
            dma((1,)),
            dma((2,)),
            dma((1,)),
        ],
        compiler_params=pltpu.CompilerParams(
            collective_id=0, has_side_effects=True, vmem_limit_bytes=60 * 1024 * 1024
        ),
    )(
        cond_latent.reshape(depth // HEAD, HEAD),
        cond_context.reshape(depth // HEAD, HEAD),
        norm_gain.reshape(1, depth),
        q_gain.reshape(1, HEAD),
        k_gain.reshape(1, HEAD),
        latent,
        context,
        w_shift,
        w_scale,
        w_gate,
        w_query,
        w_key,
        w_value,
        w_out,
    )


def solution(mesh):
    placed = (
        P(("grp", "sp"), None),
        P(("grp", "sp"), None),
        P("grp"),
        P(),
        P("sp", "tp"),
        P("sp", "tp"),
        P("sp", "tp"),
        P(),
        P(None, "tp"),
        P(None, "tp"),
        P(None, "tp"),
        P(),
        P(),
        P("tp", None),
    )
    return jax.shard_map(
        functools.partial(body, mesh.shape["grp"], mesh.shape["sp"], mesh.shape["tp"]),
        mesh=mesh,
        in_specs=placed,
        out_specs=P(("grp", "sp", "tp"), None),
        check_vma=False,
    )
```

```python
import functools
import math

import jax
import jax.numpy as jnp
from jax import lax
from jax.experimental import pallas as pl
from jax.experimental.pallas import tpu as pltpu
from jax.sharding import PartitionSpec as P

HEADS = 16
KV_HEADS = 8
HEAD = 128
GRID_W = 64
GROUP = HEADS // KV_HEADS

epsilon = 1e-06
context_lift = 1.5
rope_theta = 10000.0

MESH = pl.DeviceIdType.MESH
f32 = jnp.float32
bf16 = jnp.bfloat16


def tile_of(rows, most):
    best = 16
    for size in range(16, most + 1, 16):
        if rows % size == 0:
            best = size
    return best


def kernel(
    n_grp,
    n_sp,
    n_tp,
    tok,
    ctx,
    share,
    cond_latent_hbm,
    cond_context_hbm,
    gain_hbm,
    q_gain_hbm,
    k_gain_hbm,
    latent_hbm,
    context_hbm,
    w_shift_hbm,
    w_scale_hbm,
    w_gate_hbm,
    w_query_hbm,
    w_key_hbm,
    w_value_hbm,
    w_out_hbm,
    out_hbm,
    cond_latent_ref,
    cond_context_ref,
    gain_ref,
    q_gain_ref,
    k_gain_ref,
    out_ref,
    act_ref,
    x,
    w_mod,
    w_query,
    w_key,
    w_value,
    w_all,
    w_rest,
    inv,
    cos_ref,
    sin_a_ref,
    sin_b_ref,
    part,
    part_in,
    summed,
    mod,
    gate_part,
    gate_in,
    gate_sum,
    gate_mod,
    queries,
    kv,
    top,
    total,
    acc,
    attended,
    att_all,
    acc_out,
    pair_out,
    pair_in,
    mine,
    far_out,
    far_in,
    load_sem,
    mod_send,
    mod_recv,
    mod2_send,
    mod2_recv,
    gate_send,
    gate_recv,
    gate2_send,
    gate2_recv,
    right_send,
    right_recv,
    left_send,
    left_recv,
    pair_send,
    pair_recv,
    far_send,
    far_recv,
    own_send,
    own_recv,
    across_send,
    across_recv,
    beside_send,
    beside_recv,
    over_send,
    over_recv,
    last_send,
    last_recv,
    att_send,
    att_recv,
    out_sem,
):
    grp = lax.axis_index("grp")
    sp = lax.axis_index("sp")
    tp = lax.axis_index("tp")
    chips = n_tp // 2
    chip = tp // 2
    core = lax.rem(tp, 2)
    partner = chip * 2 + 1 - core
    piece = tok // n_tp
    turns = w_all.shape[2] // (n_grp * share)
    shared = w_all.shape[2]
    mod_rows = w_mod.shape[1]
    rows = tok + ctx
    depth = x.shape[1]
    mod_cols = mod.shape[2]
    heads = queries.shape[1] // HEAD
    kv_cols = kv.shape[2] // 2
    kv_heads = kv_cols // HEAD
    kv_tile = tile_of(rows, 128)
    kv_chunks = rows // kv_tile
    per_unit = 2 if kv_chunks % 2 == 0 else 1
    units = kv_chunks // per_unit
    unit_rows = kv_tile * per_unit

    loads = {}

    def load(name, index, source, target):
        loads[name] = pltpu.make_async_copy(source, target, load_sem.at[index])
        loads[name].start()

    load("cond_latent", 10, cond_latent_hbm, cond_latent_ref)
    load("cond_context", 11, cond_context_hbm, cond_context_ref)
    load("shift", 0, w_shift_hbm, w_mod.at[0])
    load("scale", 1, w_scale_hbm, w_mod.at[1])
    load("latent", 3, latent_hbm, x.at[pl.ds(0, tok)])
    load("context", 4, context_hbm, x.at[pl.ds(tok, ctx)])
    load("gain", 12, gain_hbm, gain_ref)
    load("q_gain", 13, q_gain_hbm, q_gain_ref)
    load("k_gain", 14, k_gain_hbm, k_gain_ref)

    barrier = pltpu.get_barrier_semaphore()
    for k in range(1, n_sp):
        pl.semaphore_signal(
            barrier, inc=1, device_id={"sp": lax.rem(sp + k, n_sp)}, device_id_type=MESH
        )
    for k in range(1, n_tp):
        pl.semaphore_signal(
            barrier, inc=1, device_id={"tp": lax.rem(tp + k, n_tp)}, device_id_type=MESH
        )

    for k in range(1, n_grp):
        pl.semaphore_signal(
            barrier, inc=1, device_id={"grp": lax.rem(grp + k, n_grp)}, device_id_type=MESH
        )

    loads["cond_latent"].wait()
    loads["cond_context"].wait()
    vectors = [ref[...].astype(f32) for ref in (cond_latent_ref, cond_context_ref)]
    vectors = [vector * (1.0 / (1.0 + jnp.exp(-vector))) for vector in vectors]
    lane_rows = depth // HEAD
    for j in range(lane_rows):
        pair = [vector[j : j + 1, :] for vector in vectors]
        act_ref[0:2, j * HEAD : (j + 1) * HEAD] = jnp.concatenate(pair, axis=0)
    mine_at = pl.ds(pl.multiple_of(sp * mod_rows, 128), mod_rows)
    act = act_ref[:, mine_at]
    act_row = lax.broadcasted_iota(jnp.int32, act.shape, 0)
    act = jnp.where(act_row < 2, act, 0.0).astype(bf16)
    for which, name in enumerate(("shift", "scale")):
        loads[name].wait()
        got = jnp.dot(act, w_mod[which], preferred_element_type=f32)
        part[2 * which : 2 * which + 2, :] = got[0:2, :]
    pl.semaphore_wait(barrier, n_grp + n_sp + n_tp - 3)

    def all_of(held, send, recv):
        return pltpu.make_async_remote_copy(
            src_ref=held,
            dst_ref=held,
            send_sem=send,
            recv_sem=recv,
            device_id={"tp": partner},
            device_id_type=MESH,
        )

    def mod_copy(k):
        return pltpu.make_async_remote_copy(
            src_ref=part,
            dst_ref=part_in.at[k - 1],
            send_sem=mod_send.at[0],
            recv_sem=mod_recv.at[0],
            device_id={"sp": lax.rem(sp + k, n_sp)},
            device_id_type=MESH,
        )

    for k in range(1, n_sp):
        mod_copy(k).start()
    load("gate", 2, w_gate_hbm, w_mod.at[2])
    load("key", 5, w_key_hbm, w_key)
    load("value", 6, w_value_hbm, w_value)
    load("query", 7, w_query_hbm, w_query)
    load("out", 8, w_out_hbm.at[:, pl.ds(0, shared)], w_all.at[tp])
    load("rest", 9, w_out_hbm.at[:, pl.ds(shared, depth - shared)], w_rest)

    def columns_of(group, i):
        return pl.ds(pl.multiple_of((i * n_grp + group) * share, 128), share)

    def source(k, which):
        return lax.rem(chip - k + chips, chips) * 2 + which

    def beside_own():
        return pltpu.make_async_remote_copy(
            src_ref=w_out_hbm.at[:, pl.ds(0, shared)],
            dst_ref=w_all.at[tp],
            send_sem=own_send.at[0],
            recv_sem=own_recv.at[0],
            device_id={"tp": partner},
            device_id_type=MESH,
        )

    def across(k, i):
        cols = columns_of(grp, i)
        return pltpu.make_async_remote_copy(
            src_ref=w_out_hbm.at[:, cols],
            dst_ref=w_all.at[tp, :, cols],
            send_sem=across_send.at[0],
            recv_sem=across_recv.at[k - 1, i],
            device_id={"tp": lax.rem(chip + k, chips) * 2 + core},
            device_id_type=MESH,
        )

    def relay(held, send, recv, to):
        return pltpu.make_async_remote_copy(
            src_ref=held,
            dst_ref=held,
            send_sem=send,
            recv_sem=recv,
            device_id=to,
            device_id_type=MESH,
        )

    in_block = pair_out.shape[3] // (n_grp * share)
    tail_from = turns - in_block

    def batch_of(i):
        return 0 if i < tail_from else 1

    def beside(k, i, which=None):
        which = core if which is None else which
        held = w_all.at[source(k, which), :, columns_of(grp, i)]
        return relay(
            held, beside_send.at[0], beside_recv.at[batch_of(i)], {"tp": partner}
        )

    def over(j, k, i, group=None):
        group = grp if group is None else group
        held = w_all.at[source(k, core), :, columns_of(group, i)]
        return relay(
            held,
            over_send.at[0],
            over_recv.at[j - 1, k - 1, i],
            {"grp": lax.rem(grp + j, n_grp)},
        )

    def last(j, k, i, which=None):
        which = core if which is None else which
        group = lax.rem(grp - j + n_grp, n_grp)
        held = w_all.at[source(k, which), :, columns_of(group, i)]
        return relay(
            held,
            last_send.at[0],
            last_recv.at[batch_of(i)],
            {"tp": partner},
        )

    def pass_on(i):
        for k in range(1, chips):
            across(k, i).wait_recv()
            for j in range(1, n_grp):
                over(j, k, i).start()
            beside(k, i).start()

    def pass_over(i):
        for j in range(1, n_grp):
            for k in range(1, chips):
                over(j, k, i, lax.rem(grp - j + n_grp, n_grp)).wait_recv()
                last(j, k, i).start()


    loads["latent"].wait()
    loads["context"].wait()

    def stats(i, carry):
        at = pl.ds(pl.multiple_of(i * 16, 16), 16)
        piece = x[at, :].astype(f32)
        inv[at, :] = lax.rsqrt(jnp.mean(piece * piece, axis=-1, keepdims=True) + epsilon)
        return carry

    lax.fori_loop(0, rows // 16, stats, 0, unroll=2)

    all_of(part_in, mod_send.at[0], mod_recv.at[0]).wait_recv()
    whole = part[...]
    for k in range(1, n_sp):
        whole = whole + part_in[k - 1]
    summed[...] = whole
    mod[tp] = whole

    def mod2_copy(k):
        return pltpu.make_async_remote_copy(
            src_ref=summed,
            dst_ref=mod.at[tp],
            send_sem=mod2_send.at[0],
            recv_sem=mod2_recv.at[0],
            device_id={"tp": lax.rem(tp + k, n_tp)},
            device_id_type=MESH,
        )

    for k in range(1, n_tp):
        mod2_copy(k).start()
    beside_own().start()
    for i in range(turns):
        for k in range(1, chips):
            across(k, i).start()

    def gate_copy(k):
        return pltpu.make_async_remote_copy(
            src_ref=gate_part,
            dst_ref=gate_in.at[k - 1],
            send_sem=gate_send.at[0],
            recv_sem=gate_recv.at[0],
            device_id={"sp": lax.rem(sp + k, n_sp)},
            device_id_type=MESH,
        )

    def gate2_copy(k):
        return pltpu.make_async_remote_copy(
            src_ref=gate_sum,
            dst_ref=gate_mod.at[tp],
            send_sem=gate2_send.at[0],
            recv_sem=gate2_recv.at[0],
            device_id={"tp": lax.rem(tp + k, n_tp)},
            device_id_type=MESH,
        )

    loads["gate"].wait()
    gate_part[...] = jnp.dot(act, w_mod[2], preferred_element_type=f32)[0:2, :]
    for k in range(1, n_sp):
        gate_copy(k).start()
    def tables(i, carry):
        at = pl.ds(pl.multiple_of(i * 16, 16), 16)
        index = i * 16 + lax.broadcasted_iota(jnp.int32, (16, HEAD), 0)
        lane = lax.broadcasted_iota(jnp.int32, (16, HEAD), 1)
        freqs = HEAD // 4
        position = sp * tok + index
        inverse = jnp.exp(lax.rem(lane, freqs).astype(f32) * (-math.log(rope_theta) / freqs))
        place = jnp.where(lane < 2 * freqs, lax.div(position, GRID_W), lax.rem(position, GRID_W))
        angle = jnp.where(index < tok, place.astype(f32) * inverse, 0.0)
        sine = jnp.sin(angle)
        first_half = lax.rem(lax.div(lane, freqs), 2) == 0
        cos_ref[at, :] = jnp.cos(angle)
        sin_a_ref[at, :] = jnp.where(first_half, -sine, 0.0)
        sin_b_ref[at, :] = jnp.where(first_half, 0.0, sine)
        return carry

    lax.fori_loop(0, rows // 16, tables, 0)
    all_of(mod.at[pl.ds(0, n_tp - 1)], mod2_send.at[0], mod2_recv.at[0]).wait_recv()
    for name in ("gain", "q_gain", "k_gain"):
        loads[name].wait()

    def normalize(low, high):
        for j in range(n_tp):
            cols = slice(j * mod_cols, (j + 1) * mod_cols)
            for row, first, end in ((0, low, min(high, tok)), (1, max(low, tok), high)):
                if first < end:
                    factor = gain_ref[:, cols] * (1.0 + mod[j, 2 + row : 3 + row, :])
                    shift = mod[j, row : row + 1, :]
                    for start in range(first, end, 16):
                        at = slice(start, start + 16)
                        piece = x[at, cols].astype(f32)
                        x[at, cols] = (piece * inv[at, :] * factor + shift).astype(bf16)

    def turn(vector, gain, at):
        vector = vector * lax.rsqrt(jnp.mean(vector * vector, axis=-1, keepdims=True) + epsilon) * gain
        ahead = pltpu.roll(vector, HEAD - HEAD // 4, 1)
        behind = pltpu.roll(vector, HEAD // 4, 1)
        return vector * cos_ref[at, :] + ahead * sin_a_ref[at, :] + behind * sin_b_ref[at, :]

    def stream_copy(block, step, c, send, recv, to):
        held = kv.at[block, pl.ds(pl.multiple_of(c * kv_tile, 16), kv_tile)]
        return pltpu.make_async_remote_copy(
            src_ref=held,
            dst_ref=held,
            send_sem=send.at[0],
            recv_sem=recv.at[step, c],
            device_id={"sp": to},
            device_id_type=MESH,
        )

    to_right = jnp.minimum(sp + 1, n_sp - 1)
    to_left = jnp.maximum(sp - 1, 0)

    def right_copy(step, c):
        return stream_copy(jnp.maximum(sp - step, 0), step, c, right_send, right_recv, to_right)

    def left_copy(step, c):
        return stream_copy(jnp.minimum(sp + step, n_sp - 1), step, c, left_send, left_recv, to_left)

    def right_arrival(step, c):
        return stream_copy(jnp.maximum(sp - 1 - step, 0), step, c, right_send, right_recv, to_right)

    def left_arrival(step, c):
        return stream_copy(
            jnp.minimum(sp + 1 + step, n_sp - 1), step, c, left_send, left_recv, to_left
        )

    def early_pass(act_on, i):
        if i < turns:
            act_on(i)

    for c in range(kv_chunks):
        low, high = c * kv_tile, (c + 1) * kv_tile
        at = slice(low, high)
        normalize(low, high)
        if c == 0:
            loads["key"].wait()
            loads["value"].wait()
        raw = jnp.dot(x[at, :], w_key[...], preferred_element_type=f32)
        raw_values = jnp.dot(x[at, :], w_value[...], preferred_element_type=f32)
        for h in range(kv_heads):
            cols = slice(h * HEAD, (h + 1) * HEAD)
            kv[sp, at, cols] = turn(raw[:, cols], k_gain_ref[...], at).astype(bf16)
        kv[sp, at, kv_cols:] = raw_values.astype(bf16)

        @pl.when(sp < n_sp - 1)
        def _():
            right_copy(0, c).start()

        @pl.when(sp > 0)
        def _():
            left_copy(0, c).start()

        if c == min(1, kv_chunks - 1):
            early_pass(pass_on, 0)

    early_pass(pass_on, 1)
    q_tile = tile_of(tok, 256)

    def project_queries(i, carry):
        at = pl.ds(pl.multiple_of(i * q_tile, 16), q_tile)
        raw = jnp.dot(x[at, :], w_query[...], preferred_element_type=f32)
        for h in range(heads):
            cols = slice(h * HEAD, (h + 1) * HEAD)
            queries[at, cols] = turn(raw[:, cols], q_gain_ref[...], at).astype(bf16)
        return carry

    stream = (n_sp - 1) * kv_chunks

    def serve(j):
        step = j // kv_chunks
        c = lax.rem(j, kv_chunks)

        @pl.when(jnp.logical_and(j < stream, jnp.logical_and(sp - 1 - step >= 0, sp < n_sp - 1)))
        def _():
            right_arrival(step, c).wait_recv()
            right_copy(step + 1, c).start()

        @pl.when(jnp.logical_and(j < stream, jnp.logical_and(sp + 1 + step <= n_sp - 1, sp > 0)))
        def _():
            left_arrival(step, c).wait_recv()
            left_copy(step + 1, c).start()

    loads["query"].wait()
    q_steps = tok // q_tile
    for i in range(q_steps):
        project_queries(i, 0)
        if i == max(q_steps - 2, 0):
            serve(jnp.int32(0))
    serve(jnp.int32(1))

    scaling = HEAD ** (-0.5)
    a_tile = tile_of(tok, 128)

    def attend(block, unit, first, size=None):
        size = unit_rows if size is None else size
        held = pl.ds(pl.multiple_of(unit * size, 16), size)
        lane = unit * size + lax.broadcasted_iota(jnp.int32, (1, size), 1)
        lift = jnp.where(lane >= tok, context_lift, 0.0).astype(f32)
        spans = [slice(h * HEAD, (h + 1) * HEAD) for h in range(heads)]

        def one(i, carry):
            at = pl.ds(pl.multiple_of(i * a_tile, 16), a_tile)
            scores = []
            for h in range(heads):
                kv_span = slice((h // GROUP) * HEAD, (h // GROUP + 1) * HEAD)
                scores.append(
                    lax.dot_general(
                        queries[at, spans[h]],
                        kv[block, held, kv_span],
                        (((1,), (1,)), ((), ())),
                        preferred_element_type=f32,
                    )
                    * scaling
                    + lift
                )
            highs, fades, sums, products = [], [], [], []
            for h in range(heads):
                high = jnp.max(scores[h], axis=-1, keepdims=True)
                if not first:
                    old = top[h, at, :]
                    high = jnp.maximum(high, old)
                    fades.append(jnp.exp(old - high))
                highs.append(high)
                weights = jnp.exp(scores[h] - high)
                sums.append(jnp.sum(weights, axis=-1, keepdims=True))
                begin = kv_cols + (h // GROUP) * HEAD
                products.append(
                    jnp.dot(
                        weights.astype(bf16),
                        kv[block, held, begin : begin + HEAD],
                        preferred_element_type=f32,
                    )
                )
            if not first:
                sums = [total[h, at, :] * fades[h] + sums[h] for h in range(heads)]
                products = [acc[at, spans[h]] * fades[h] + products[h] for h in range(heads)]
            for h in range(heads):
                top[h, at, :] = highs[h]
                total[h, at, :] = sums[h]
                acc[at, spans[h]] = products[h]
            return carry

        lax.fori_loop(0, tok // a_tile, one, 0, unroll=True)

    early_pass(pass_on, 2)
    attend(sp, 0, True)
    early_pass(pass_over, 0)
    serve(jnp.int32(2))
    for unit in range(1, units):
        attend(sp, unit, False)
    serve(jnp.int32(3))
    ahead = 4
    early_pass(pass_on, 3)
    early_pass(pass_over, 1)

    all_of(gate_in, gate_send.at[0], gate_recv.at[0]).wait_recv()
    gate_whole = gate_part[...]
    for k in range(1, n_sp):
        gate_whole = gate_whole + gate_in[k - 1]
    gate_sum[...] = gate_whole
    gate_mod[tp] = gate_whole
    for k in range(1, n_tp):
        gate2_copy(k).start()
    steps = (n_sp - 1) * units
    events = {}
    halves = 2 * steps
    for i in range(4, turns):
        at = (0, 1, 2, 3, 5, 7, 9, 11)[i - 4] if i < 12 else i
        events.setdefault(min(at, halves - 1), []).append((pass_on, i))
    for i in range(2, turns):
        at = (1, 3, 4, 5, 6, 8, 10)[i - 2] if i < 9 else halves
        events.setdefault(min(at, halves), []).append((pass_over, i))

    def take_events(t, half):
        for at in sorted(events):
            if at < halves and at % 2 == half:

                @pl.when(t == at // 2)
                def _():
                    for act_on, i in events[at]:
                        act_on(i)

    def gather_step(t, carry):
        step = t // units
        unit = lax.rem(t, units)
        from_left = sp - 1 - step >= 0
        from_right = sp + 1 + step <= n_sp - 1
        per = per_unit
        for k in range((per + 1) // 2):
            serve(ahead + t * per + k)

        @pl.when(from_left)
        def _():
            @pl.when(sp == n_sp - 1)
            def _():
                for k in range(per):
                    right_arrival(step, unit * per + k).wait_recv()

            attend(jnp.maximum(sp - 1 - step, 0), unit, False)

        for k in range((per + 1) // 2, per):
            serve(ahead + t * per + k)

        take_events(t, 0)

        @pl.when(from_right)
        def _():
            @pl.when(sp == 0)
            def _():
                for k in range(per):
                    left_arrival(step, unit * per + k).wait_recv()

            attend(jnp.minimum(sp + 1 + step, n_sp - 1), unit, False)

        take_events(t, 1)
        return carry

    lax.fori_loop(0, steps - 1, gather_step, 0)
    take_events(jnp.int32(steps - 1), 0)
    for k in range(per_unit):
        c = (units - 1) * per_unit + k

        @pl.when(sp == n_sp - 1)
        def _():
            right_arrival(n_sp - 2, c).wait_recv()
            attend(0, c, False, kv_tile)

        @pl.when(sp == 0)
        def _():
            left_arrival(n_sp - 2, c).wait_recv()
            attend(n_sp - 1, c, False, kv_tile)

    take_events(jnp.int32(steps - 1), 1)

    def att_copy(k):
        to = lax.rem(tp + k, n_tp)
        return pltpu.make_async_remote_copy(
            src_ref=attended.at[pl.ds(pl.multiple_of(to * piece, 16), piece)],
            dst_ref=att_all.at[tp],
            send_sem=att_send.at[0],
            recv_sem=att_recv.at[jnp.where(to == partner, 0, 1)],
            device_id={"tp": to},
            device_id_type=MESH,
        )

    def finish(k):
        at = pl.ds(pl.multiple_of(lax.rem(tp + k, n_tp) * piece, 16), piece)
        for h in range(heads):
            cols = slice(h * HEAD, (h + 1) * HEAD)
            attended[at, cols] = (acc[at, cols] / total[h, at, :]).astype(bf16)

    for k in range(2, n_tp + 2):
        finish(k)
        if k % n_tp:
            att_copy(k % n_tp).start()
    att_all[tp] = attended[pl.ds(pl.multiple_of(tp * piece, 16), piece), :]
    late = events.get(halves, [])
    width = pair_out.shape[3]
    chunks = pair_out.shape[1]

    def pair_copy(k, c):
        return pltpu.make_async_remote_copy(
            src_ref=pair_out.at[k, c],
            dst_ref=pair_in.at[k, c],
            send_sem=pair_send.at[0],
            recv_sem=pair_recv.at[k, c],
            device_id={"tp": partner},
            device_id_type=MESH,
        )

    def far_copy(k, c):
        return pltpu.make_async_remote_copy(
            src_ref=far_out.at[k - 1, c],
            dst_ref=far_in.at[k - 1, c],
            send_sem=far_send.at[0],
            recv_sem=far_recv.at[k - 1, c],
            device_id={"tp": lax.rem(chip + k, chips) * 2 + core},
            device_id_type=MESH,
        )

    def multiply(k, c):
        to = lax.rem(chip + k, chips)
        cols = pl.ds(pl.multiple_of(c * width, width), width)

        def part_of(which):
            at = pl.ds(pl.multiple_of((to * 2 + which) * piece, 16), piece)
            return jnp.dot(
                attended[at, :], w_rest[:, cols], preferred_element_type=f32
            ).astype(bf16)

        pair_out[k, c] = part_of(1 - core)
        pair_copy(k, c).start()
        mine[k, c] = part_of(core)

    def combine(k, c):
        pair_copy(k, c).wait_recv()
        far_out[k - 1, c] = (mine[k, c].astype(f32) + pair_in[k, c].astype(f32)).astype(bf16)
        far_copy(k, c).start()

    blocks = shared // width

    def product(source_at, cols):
        return (
            jnp.dot(att_all[source_at], w_all[source_at, :, cols], preferred_element_type=f32)
            .astype(bf16)
            .astype(f32)
        )

    loads["rest"].wait()
    loads["out"].wait()
    for k in range(1, chips):
        for c in range(chunks):
            multiply(k, c)
    for c in range(blocks):
        cols = slice(c * width, (c + 1) * width)
        acc_out[:, cols] = product(tp, cols)
    for k in range(1, chips):
        for c in range(chunks):
            combine(k, c)
    for c in range(chunks):
        multiply(0, c)
    beside_own().wait_recv()
    all_of(att_all.at[pl.ds(0, 1)], att_send.at[0], att_recv.at[0]).wait_recv()
    for c in range(blocks):
        cols = slice(c * width, (c + 1) * width)
        acc_out[:, cols] += product(partner, cols)
    for act_on, i in late:
        act_on(i)
    if chips > 1:
        all_of(att_all.at[pl.ds(0, n_tp - 2)], att_send.at[0], att_recv.at[1]).wait_recv()

    all_of(gate_mod.at[pl.ds(0, n_tp - 1)], gate2_send.at[0], gate2_recv.at[0]).wait_recv()
    per = mod_cols // width

    def put(at, result):
        cols = slice(at * width, (at + 1) * width)
        first = (at % per) * width
        gate = gate_mod[at // per, 0:1, first : first + width]
        out_ref[:, cols] = (gate * result).astype(bf16)
        out_copy(at).start()

    def out_copy(at):
        cols = pl.ds(at * width, width)
        return pltpu.make_async_copy(out_ref.at[:, cols], out_hbm.at[:, cols], out_sem.at[0])

    for c in range(blocks):
        if chips > 1 and c in (0, blocks - 1):
            batch = 0 if c == 0 and blocks > 1 else 1
            count = (tail_from if batch == 0 else in_block) * share
            for copies, sems in ((1, beside_recv), (n_grp - 1, last_recv)):
                if copies * count:
                    held = w_all.at[pl.ds(0, chips - 1), :, pl.ds(0, copies * count)]
                    all_of(held, own_send.at[0], sems.at[batch]).wait_recv()
        cols = slice(c * width, (c + 1) * width)
        result = acc_out[:, cols]
        for k in range(1, chips):
            for which in range(2):
                result = result + product(source(k, which), cols)
        put(c, result)
    for c in range(chunks):
        pair_copy(0, c).wait_recv()
        result = mine[0, c].astype(f32) + pair_in[0, c].astype(f32)
        for k in range(1, chips):
            far_copy(k, c).wait_recv()
            result = result + far_in[k - 1, c].astype(f32)
        put(blocks + c, result)

    beside_own().wait_send()
    all_of(att_all.at[pl.ds(0, n_tp - 1)], att_send.at[0], att_recv.at[0]).wait_send()
    if chips > 1:
        count = turns * share
        held = w_all.at[pl.ds(0, chips - 1), :, pl.ds(0, count)]
        all_of(held, across_send.at[0], own_recv.at[0]).wait_send()
        all_of(held, beside_send.at[0], own_recv.at[0]).wait_send()
        if n_grp > 1:
            held = w_all.at[pl.ds(0, chips - 1), :, pl.ds(0, (n_grp - 1) * count)]
            all_of(held, over_send.at[0], own_recv.at[0]).wait_send()
            all_of(held, last_send.at[0], own_recv.at[0]).wait_send()
    all_of(part_in, mod_send.at[0], mod_recv.at[0]).wait_send()
    all_of(gate_in, gate_send.at[0], gate_recv.at[0]).wait_send()
    all_of(mod.at[pl.ds(0, n_tp - 1)], mod2_send.at[0], mod2_recv.at[0]).wait_send()
    all_of(gate_mod.at[pl.ds(0, n_tp - 1)], gate2_send.at[0], gate2_recv.at[0]).wait_send()

    for at in range(n_sp):

        @pl.when(sp == at)
        def _():
            if at < n_sp - 1:
                all_of(kv.at[pl.ds(0, at + 1)], right_send.at[0], right_recv.at[0, 0]).wait_send()
            if at > 0:
                all_of(kv.at[pl.ds(0, n_sp - at)], left_send.at[0], left_recv.at[0, 0]).wait_send()

    all_of(pair_out, pair_send.at[0], pair_recv.at[0, 0]).wait_send()
    if chips > 1:
        all_of(far_out, far_send.at[0], far_recv.at[0, 0]).wait_send()
    pltpu.make_async_copy(out_ref, out_hbm, out_sem.at[0]).wait()


def body(
    n_grp,
    n_sp,
    n_tp,
    latent,
    context,
    cond_latent,
    cond_context,
    w_shift,
    w_scale,
    w_gate,
    norm_gain,
    w_query,
    w_key,
    w_value,
    q_gain,
    k_gain,
    w_out,
):
    tok, depth = latent.shape
    ctx = context.shape[0]
    rows = tok + ctx
    mod_rows, mod_cols = w_shift.shape
    chips = n_tp // 2
    piece = tok // n_tp
    width = min(512, mod_cols)
    share = min(128, width)
    turns = (3 * depth // 4) // (n_grp * share)
    shared = turns * n_grp * share
    shared -= shared % width
    turns = shared // (n_grp * share)
    chunks = (depth - shared) // width
    kv_cols = w_key.shape[1]
    q_cols = w_query.shape[1]
    heads = q_cols // HEAD
    hbm = pl.BlockSpec(memory_space=pl.ANY)
    dma = pltpu.SemaphoreType.DMA
    far = max(chips - 1, 1)
    others = max(n_grp - 1, 1)
    kv_chunks = rows // tile_of(rows, 128)
    return pl.pallas_call(
        functools.partial(kernel, n_grp, n_sp, n_tp, tok, ctx, share),
        out_shape=jax.ShapeDtypeStruct((piece, depth), bf16),
        in_specs=[hbm] * 14,
        out_specs=hbm,
        scratch_shapes=[
            pltpu.VMEM((depth // HEAD, HEAD), bf16),
            pltpu.VMEM((depth // HEAD, HEAD), bf16),
            pltpu.VMEM((1, depth), f32),
            pltpu.VMEM((1, HEAD), f32),
            pltpu.VMEM((1, HEAD), f32),
            pltpu.VMEM((piece, depth), bf16),
            pltpu.VMEM((16, depth), f32),
            pltpu.VMEM((rows, depth), bf16),
            pltpu.VMEM((3, mod_rows, mod_cols), bf16),
            pltpu.VMEM(w_query.shape, bf16),
            pltpu.VMEM(w_key.shape, bf16),
            pltpu.VMEM(w_value.shape, bf16),
            pltpu.VMEM((n_tp, w_out.shape[0], shared), bf16),
            pltpu.VMEM((w_out.shape[0], depth - shared), bf16),
            pltpu.VMEM((rows, 1), f32),
            pltpu.VMEM((rows, HEAD), f32),
            pltpu.VMEM((rows, HEAD), f32),
            pltpu.VMEM((rows, HEAD), f32),
            pltpu.VMEM((4, mod_cols), f32),
            pltpu.VMEM((n_sp - 1, 4, mod_cols), f32),
            pltpu.VMEM((4, mod_cols), f32),
            pltpu.VMEM((n_tp, 4, mod_cols), f32),
            pltpu.VMEM((2, mod_cols), f32),
            pltpu.VMEM((n_sp - 1, 2, mod_cols), f32),
            pltpu.VMEM((2, mod_cols), f32),
            pltpu.VMEM((n_tp, 2, mod_cols), f32),
            pltpu.VMEM((tok, q_cols), bf16),
            pltpu.VMEM((n_sp, rows, 2 * kv_cols), bf16),
            pltpu.VMEM((heads, tok, 1), f32),
            pltpu.VMEM((heads, tok, 1), f32),
            pltpu.VMEM((tok, q_cols), f32),
            pltpu.VMEM((tok, q_cols), bf16),
            pltpu.VMEM((n_tp, piece, q_cols), bf16),
            pltpu.VMEM((piece, shared), f32),
            pltpu.VMEM((chips, chunks, piece, width), bf16),
            pltpu.VMEM((chips, chunks, piece, width), bf16),
            pltpu.VMEM((chips, chunks, piece, width), bf16),
            pltpu.VMEM((far, chunks, piece, width), bf16),
            pltpu.VMEM((far, chunks, piece, width), bf16),
            dma((15,)),
            dma((1,)),
            dma((1,)),
            dma((1,)),
            dma((1,)),
            dma((1,)),
            dma((1,)),
            dma((1,)),
            dma((1,)),
            dma((1,)),
            dma((n_sp - 1, kv_chunks)),
            dma((1,)),
            dma((n_sp - 1, kv_chunks)),
            dma((1,)),
            dma((chips, chunks)),
            dma((1,)),
            dma((far, chunks)),
            dma((1,)),
            dma((1,)),
            dma((1,)),
            dma((far, turns)),
            dma((1,)),
            dma((2,)),
            dma((1,)),
            dma((others, far, turns)),
            dma((1,)),
            dma((2,)),
            dma((1,)),
            dma((2,)),
            dma((1,)),
        ],
        compiler_params=pltpu.CompilerParams(
            collective_id=0, has_side_effects=True, vmem_limit_bytes=60 * 1024 * 1024
        ),
    )(
        cond_latent.reshape(depth // HEAD, HEAD),
        cond_context.reshape(depth // HEAD, HEAD),
        norm_gain.reshape(1, depth),
        q_gain.reshape(1, HEAD),
        k_gain.reshape(1, HEAD),
        latent,
        context,
        w_shift,
        w_scale,
        w_gate,
        w_query,
        w_key,
        w_value,
        w_out,
    )


def solution(mesh):
    placed = (
        P(("grp", "sp"), None),
        P(("grp", "sp"), None),
        P("grp"),
        P(),
        P("sp", "tp"),
        P("sp", "tp"),
        P("sp", "tp"),
        P(),
        P(None, "tp"),
        P(None, "tp"),
        P(None, "tp"),
        P(),
        P(),
        P("tp", None),
    )
    return jax.shard_map(
        functools.partial(body, mesh.shape["grp"], mesh.shape["sp"], mesh.shape["tp"]),
        mesh=mesh,
        in_specs=placed,
        out_specs=P(("grp", "sp", "tp"), None),
        check_vma=False,
    )
```
